256 devices in a mesh: sp: 32 (over z, y), tp: 8 (over x, core).
Axes of the slice: x: 4, y: 4, z: 8, core: 2. Of those that a mesh axis runs over, the one named last changes fastest.
Arguments:
- resid: bfloat16 [16384, 2048], P('sp', 'tp'), may hold values from -41 to 41
- queries: bfloat16 [16384, 1024], P('sp', 'tp'), may hold values from -6 to 6
- keys: bfloat16 [16384, 1024], P('sp', 'tp'), may hold values from -6 to 6
- values: bfloat16 [16384, 1024], P('sp', 'tp'), may hold values from -6 to 6
- mix_lambda: float32 [8], P('tp'), may hold values from 0.3 to 0.8
- head_gain: float32 [128], replicated, may hold values from 0.1 to 1.9
- out_weight: bfloat16 [1024, 2048], P(None, 'tp'), may hold values from -0.1875 to 0.1875
- norm_gain: float32 [2048], P('tp'), may hold values from 0.1 to 1.9
- gate_weight: bfloat16 [2048, 5632], P('sp', 'tp'), may hold values from -0.125 to 0.125
- up_weight: bfloat16 [2048, 5632], P('sp', 'tp'), may hold values from -0.125 to 0.125
- conv_weight: float32 [3, 5632], P(None, 'tp'), may hold values from -3.5 to 3.5
- conv_bias: float32 [5632], P('tp'), may hold values from -3 to 3
- down_weight: bfloat16 [5632, 2048], P('tp', 'sp'), may hold values from -0.078125 to 0.078125
Outputs:
- layer_out: bfloat16 [16384, 2048], P('sp', 'tp')
The draws below stay inside these ranges and needn't reach their ends.
All inputs are finite; a program needn't handle non-finite values.
Results may differ from the reference program's by a relative error of at most 0.009.
Values may be sent and summed in bfloat16 or wider, within the bound.
A program may use at most 128 MiB of HBM per device.

```python
import math
import jax
import jax.numpy as jnp
from jax import lax

D = 2048
HEADS = 8
HD = 64
VD = 128
FF = 5632
TOKENS = 16384
N_TP = 8


def pair_draw(key):
    width = HEADS * 2 * HD
    query_part = 1.3 * jnp.clip(jax.random.normal(jax.random.fold_in(key, 11), (TOKENS, width), jnp.float32), -4.0, 4.0)
    key_part = 1.3 * jnp.clip(jax.random.normal(jax.random.fold_in(key, 12), (TOKENS, width), jnp.float32), -4.0, 4.0)
    return (query_part, key_part)


def draw_queries(key, part):
    return pair_draw(key)[0].astype(jnp.bfloat16)


def draw_keys(key, part):
    return pair_draw(key)[1].astype(jnp.bfloat16)


def draw_resid(key, part):
    base = jax.random.fold_in(key, 21)
    row_scale = 10.0 ** (jax.random.uniform(jax.random.fold_in(base, 1), (TOKENS, 1), jnp.float32) - 0.5)
    position = jnp.arange(D, dtype=jnp.float32)[None, :] / D
    column_scale = 10.0 ** (0.7 * position + 0.3 * jax.random.uniform(jax.random.fold_in(base, 2), (1, D), jnp.float32) - 0.5)
    noise = jnp.clip(jax.random.normal(jax.random.fold_in(base, 4), (TOKENS, D), jnp.float32), -4.0, 4.0)
    return (noise * row_scale * column_scale).astype(jnp.bfloat16)


def levels(own_key, extent, pieces, smallest, high):
    loudness = 1.0
    for dim, blocks in pieces:
        steps = jax.random.uniform(jax.random.fold_in(jax.random.fold_in(own_key, 6), dim), (blocks,), jnp.float32, smallest / len(pieces), high / len(pieces))
        loudness = loudness * jnp.repeat(jnp.exp(steps), extent[dim] // blocks).reshape((-1,) + (1,) * (len(extent) - 1 - dim))
    return loudness


def normal_values(own_key, extent, scale, most, cuts=(), kind=jnp.bfloat16):
    level = levels(own_key, extent, cuts, -0.22, 0.18) if cuts else 1.0
    result = jax.random.normal(own_key, extent, jnp.float32) * scale * level
    return jnp.minimum(jnp.maximum(result, -most), most).astype(kind)


def setup_inputs(seed: int = 0) -> dict:
    arg_keys = jax.random.split(jax.random.key(seed), 14)
    resid = draw_resid(jax.random.fold_in(arg_keys[13], 71), 0)
    queries = draw_queries(jax.random.fold_in(arg_keys[13], 71), 0)
    keys = draw_keys(jax.random.fold_in(arg_keys[13], 71), 0)
    values = normal_values(arg_keys[3], (TOKENS, HEADS * VD), 1.0, 6.0, ((0, 32), (1, 8)))
    mix_lambda = jnp.clip(0.3 + 0.5 * jax.random.uniform(arg_keys[4], (HEADS,), jnp.float32) ** levels(arg_keys[4], (HEADS,), ((0, 8),), -0.2, 0.2), 0.3, 0.8)
    head_gain = jnp.clip(1.0 + 0.18 * jax.random.normal(arg_keys[5], (VD,), jnp.float32), 0.1, 1.9)
    out_weight = normal_values(arg_keys[6], (HEADS * VD, D), (HEADS * VD) ** -0.5, 0.1875, ((1, 8),))
    norm_gain = jnp.clip(1.0 + 0.18 * jax.random.normal(arg_keys[7], (D,), jnp.float32), 0.1, 1.9)
    gate_weight = normal_values(arg_keys[8], (D, FF), D ** -0.5, 0.125, ((0, 32), (1, 8)))
    up_weight = normal_values(arg_keys[9], (D, FF), D ** -0.5, 0.125, ((0, 32), (1, 8)))
    conv_weight = normal_values(arg_keys[10], (3, FF), 3 ** -0.5, 3.5, ((1, 8),), jnp.float32)
    conv_bias = normal_values(arg_keys[11], (FF,), 0.5, 3.0, ((0, 8),), jnp.float32)
    down_weight = normal_values(arg_keys[12], (FF, D), FF ** -0.5, 0.078125, ((0, 8), (1, 32)))
    return {"resid": resid, "queries": queries, "keys": keys, "values": values, "mix_lambda": mix_lambda, "head_gain": head_gain, "out_weight": out_weight, "norm_gain": norm_gain, "gate_weight": gate_weight, "up_weight": up_weight, "conv_weight": conv_weight, "conv_bias": conv_bias, "down_weight": down_weight}


def head_attention(query_head, key_head, value_head, weight_two):
    length = query_head.shape[0]
    scale = HD ** (-0.5)
    block = math.gcd(length, 512)
    query_blocks = query_head.reshape(length // block, block, 2, HD)
    key_float = key_head.astype(jnp.float32)
    value_float = value_head.astype(jnp.float32)

    def one_block(query_block):
        scores = jnp.einsum('qmd,kmd->mqk', query_block.astype(jnp.float32), key_float) * scale
        highest = lax.optimization_barrier(jnp.max(scores, axis=-1, keepdims=True))
        shifted = jnp.exp(scores - highest)
        totals = lax.optimization_barrier(jnp.sum(shifted, axis=-1))
        unnormed = lax.optimization_barrier(shifted.astype(jnp.bfloat16)).astype(jnp.float32)
        mapped = jnp.einsum('mqk,ke->mqe', unnormed, value_float) / totals[..., None]
        return mapped[0] - weight_two * mapped[1]
    return lax.map(one_block, query_blocks).reshape(length, VD)

def reference(resid, queries, keys, values, mix_lambda, head_gain, out_weight, norm_gain, gate_weight, up_weight, conv_weight, conv_bias, down_weight):
    length = queries.shape[0]
    query_heads = jnp.transpose(queries.reshape(length, HEADS, 2, HD), (1, 0, 2, 3))
    key_heads = jnp.transpose(keys.reshape(length, HEADS, 2, HD), (1, 0, 2, 3))
    value_heads = jnp.transpose(values.reshape(length, HEADS, VD), (1, 0, 2))
    mixed = lax.map(lambda parts: head_attention(parts[0], parts[1], parts[2], parts[3]), (query_heads, key_heads, value_heads, mix_lambda))
    spread = lax.optimization_barrier(jnp.mean(mixed * mixed, axis=-1, keepdims=True))
    normed = mixed * lax.rsqrt(spread + 1e-06) * head_gain * 0.8
    heads_out = jnp.transpose(normed, (1, 0, 2)).reshape(length, HEADS * VD).astype(jnp.bfloat16)
    after_mixer = resid.astype(jnp.float32) + jnp.dot(heads_out, out_weight, preferred_element_type=jnp.float32)
    squares = lax.optimization_barrier(jnp.mean(after_mixer * after_mixer, axis=-1, keepdims=True))
    normed_rows = (after_mixer * lax.rsqrt(squares + 1e-06) * norm_gain).astype(jnp.bfloat16)
    gated = jnp.dot(normed_rows, gate_weight, preferred_element_type=jnp.float32).astype(jnp.bfloat16)
    upward = jnp.dot(normed_rows, up_weight, preferred_element_type=jnp.float32)
    padded = jnp.pad(gated.astype(jnp.float32), ((1, 1), (0, 0)))
    conv = padded[:-2] * conv_weight[0] + padded[1:-1] * conv_weight[1] + padded[2:] * conv_weight[2] + conv_bias
    hidden = (jax.nn.silu(conv) * upward).astype(jnp.bfloat16)
    span = FF // N_TP
    hidden_blocks = jnp.transpose(hidden.reshape(length, N_TP, span), (1, 0, 2))
    down_blocks = down_weight.reshape(N_TP, span, D)

    def block_sum(carry, pair):
        part = jnp.dot(pair[0], pair[1], preferred_element_type=jnp.float32).astype(jnp.bfloat16)
        return (carry + part.astype(jnp.float32), None)
    mixer_out, unused = lax.scan(block_sum, jnp.zeros((length, D), jnp.float32), (hidden_blocks, down_blocks))
    return (after_mixer + mixer_out).astype(jnp.bfloat16)
```

```python
import functools

import jax
import jax.numpy as jnp
from jax import lax
from jax.experimental import pallas as pl
from jax.experimental.pallas import tpu as pltpu
from jax.sharding import PartitionSpec as P

D = 2048
HD = 64
VD = 128
LOG2E = 1.4426950408889634
NZ = 8
NY = 4
F32 = jnp.float32
BF16 = jnp.bfloat16
MESH = pl.DeviceIdType.MESH
VMEM = pl.BlockSpec(memory_space=pltpu.VMEM)
ANY = pl.BlockSpec(memory_space=pl.ANY)


def remote(src, dst, send, recv, device):
    return pltpu.make_async_remote_copy(
        src_ref=src, dst_ref=dst, send_sem=send, recv_sem=recv, device_id=device, device_id_type=MESH
    )


def meet(peers):
    barrier = pltpu.get_barrier_semaphore()
    for peer in peers:
        pl.semaphore_signal(barrier, inc=1, device_id=peer, device_id_type=MESH)
    pl.semaphore_wait(barrier, len(peers))


def attention_kernel(
    q_ref,
    k_ref,
    v_ref,
    gu_ref,
    lam_ref,
    gain_ref,
    out_ref,
    gug,
    kbuf,
    vbuf,
    qbuf,
    kk,
    vv,
    qbd,
    top,
    total,
    acc,
    osend,
    ssend,
    orecv,
    srecv,
    ks,
    kr,
    vs,
    vr,
    qs,
    qr,
    gs,
    gr,
    ya_s,
    ya_r,
    yb_s,
    yb_r,
    os,
    orr,
    ss,
    sr,
    loc,
):
    sp, tp = lax.axis_index("sp"), lax.axis_index("tp")
    z, y = sp // NY, sp % NY
    length = q_ref.shape[0]
    cols = 2 * length
    half = length // 2
    rows_g = gu_ref.shape[0]
    hg = rows_g // 2

    def index(dz, dy):
        return ((z + dz) % NZ) * NY + (y + dy) % NY

    def device(dz, dy):
        return (index(dz % NZ, dy % NY), tp)

    zr, zl = device(1, 0), device(7, 0)
    yr, yl = device(0, 1), device(0, 3)
    meet([zr, zl, yr, yl, device(0, 2)])
    started = []

    def go(copy):
        copy.start()
        started.append(copy)
        return copy

    def kslot(s):
        return k_ref if s == 0 else kbuf.at[s]

    def vslot(s):
        return v_ref if s == 0 else vbuf.at[s]

    def gslot(s, rows=None):
        if s == 0:
            return gu_ref if rows is None else gu_ref.at[rows]
        whole = gug.at[index(8 - s, 0)]
        return whole if rows is None else whole.at[rows]

    qa = [
        go(remote(q_ref, qbuf.at[1], qs.at[0], qr.at[0], yr)),
        go(remote(q_ref, qbuf.at[3], qs.at[1], qr.at[1], yl)),
    ]

    def send_kv(t):
        right, left = t, (8 - t) % 8
        out = []
        out.append(go(remote(kslot(right), kbuf.at[t + 1], ks.at[0, t], kr.at[t + 1], zr)))
        if t < 3:
            out.append(go(remote(kslot(left), kbuf.at[7 - t], ks.at[1, t], kr.at[7 - t], zl)))
            out.append(go(remote(vslot(right), vbuf.at[t + 1], vs.at[0, t], vr.at[t + 1], zr)))
        out.append(go(remote(vslot(left), vbuf.at[7 - t], vs.at[1, t], vr.at[7 - t], zl)))
        return out

    def send_g(t):
        right, left = t, (8 - t) % 8
        dst_r, dst_l = gug.at[index(8 - right, 0)], gug.at[index(8 - left, 0)]
        if t < 3:
            return [
                go(remote(gslot(right), dst_r, gs.at[0, t], gr.at[0, t], zr)),
                go(remote(gslot(left), dst_l, gs.at[1, t], gr.at[1, t], zl)),
            ]
        top_half, low_half = pl.ds(0, hg), pl.ds(hg, hg)
        return [
            go(remote(gslot(right, top_half), dst_r.at[top_half], gs.at[0, t], gr.at[0, t], zr)),
            go(remote(gslot(left, low_half), dst_l.at[low_half], gs.at[1, t], gr.at[1, t], zl)),
        ]

    def send_ya(s):
        dst = gug.at[index(8 - s, 0)]
        return [
            go(remote(gslot(s), dst, ya_s.at[0, s], ya_r.at[0, s], yr)),
            go(remote(gslot(s), dst, ya_s.at[1, s], ya_r.at[1, s], yl)),
        ]

    def send_yb(s):
        top_half, low_half = pl.ds(0, hg), pl.ds(hg, hg)
        a = gug.at[index(8 - s, 3)].at[top_half]
        b = gug.at[index(8 - s, 1)].at[low_half]
        return [
            go(remote(a, a, yb_s.at[0, s], yb_r.at[0, s], yr)),
            go(remote(b, b, yb_s.at[1, s], yb_r.at[1, s], yl)),
        ]

    def arrive(copies):
        for copy in copies:
            copy.wait_recv()

    kv = [send_kv(0)]
    g = [send_g(0)]
    own = pltpu.make_async_copy(gu_ref, gug.at[sp], loc)
    own.start()
    ya = {0: send_ya(0)}
    yb = {}

    top[...] = jnp.full(top.shape, -1e30, F32)
    total[...] = jnp.zeros(total.shape, F32)
    acc[...] = jnp.zeros(acc.shape, F32)
    row = lax.broadcasted_iota(jnp.int32, (2 * HD, 128), 0)

    def lay_queries(src, slot):
        for j in range(length // 128):
            turned = src[j * 128 : (j + 1) * 128, :].astype(F32).T * (LOG2E * HD**-0.5)
            for m in range(2):
                at = slot * cols + j * 256 + m * 128
                kept = jnp.where((row < HD) if m == 0 else (row >= HD), turned, 0.0)
                high = kept.astype(BF16)
                qbd[0:128, at : at + 128] = high
                qbd[128:256, at : at + 128] = (kept - high.astype(F32)).astype(BF16)

    def stage(slots):
        for n, s in enumerate(slots):
            kb = kslot(s)[...]
            kk[n * length : (n + 1) * length, 0:128] = kb
            kk[n * length : (n + 1) * length, 128:256] = kb
            vv[n * length : (n + 1) * length, :] = vslot(s)[...]

    def attend(count, first, last):
        keys = count * length

        def tile(i, carry):
            at = pl.ds(pl.multiple_of(i * cols, cols), cols)
            scores = jnp.dot(kk[0:keys, :], qbd[:, at], preferred_element_type=F32)
            before = top[0:1, at]
            now = jnp.maximum(before, jnp.max(scores, axis=0, keepdims=True))
            shifted = jnp.exp2(scores - now)
            factor = jnp.exp2(before - now)
            top[0:1, at] = now
            total[0:1, at] = total[0:1, at] * factor + jnp.sum(shifted, axis=0, keepdims=True)
            acc[:, at] = acc[:, at] * factor + lax.dot_general(
                vv[0:keys, :],
                shifted.astype(BF16),
                (((0,), (0,)), ((), ())),
                preferred_element_type=F32,
            )
            return carry

        lax.fori_loop(first, last, tile, 0)

    lay_queries(q_ref, 0)
    stage([0])
    attend(1, 0, 1)
    arrive(qa)
    qb = [
        go(remote(qbuf.at[1, pl.ds(0, half)], qbuf.at[2, pl.ds(0, half)], qs.at[2], qr.at[2], yr)),
        go(remote(qbuf.at[3, pl.ds(half, half)], qbuf.at[2, pl.ds(half, half)], qs.at[3], qr.at[3], yl)),
    ]
    lay_queries(qbuf.at[1], 1)
    lay_queries(qbuf.at[3], 3)
    attend(1, 1, 2)
    attend(1, 3, 4)
    arrive(qb)
    lay_queries(qbuf.at[2], 2)
    attend(1, 2, 3)

    for t in range(1, 5):
        arrive(kv[t - 1])
        if t < 4:
            kv.append(send_kv(t))
        arrive(g[t - 1])
        if t < 4:
            g.append(send_g(t))
        slots = [t, 8 - t] if t < 4 else [4]
        for s in slots:
            ya[s] = send_ya(s)
        if t == 1:
            arrive(ya[0])
            yb[0] = send_yb(0)
        else:
            for s in (t - 1, 9 - t):
                arrive(ya[s])
                yb[s] = send_yb(s)
        stage(slots)
        attend(len(slots), 0, 4)

    sent = []
    for slot in (2, 1, 3):
        at = slice(slot * cols, (slot + 1) * cols)
        scale = 1.0 / total[0:1, at]
        osend[slot] = (acc[:, at] * scale).astype(BF16)
        ssend[slot, 0:1, :] = top[0:1, at]
        ssend[slot, 1:2, :] = total[0:1, at]
        ssend[slot, 2:8, :] = jnp.zeros((6, cols), F32)
        to = device(0, 4 - slot)
        sent.append(go(remote(osend.at[slot], orecv.at[slot], os.at[slot], orr.at[slot], to)))
        sent.append(go(remote(ssend.at[slot], srecv.at[slot], ss.at[slot], sr.at[slot], to)))
    arrive(ya[4])
    yb[4] = send_yb(4)
    arrive(sent)

    tops = [top[0:1, 0:cols]] + [srecv[s, 0:1, :] for s in (1, 2, 3)]
    sums = [total[0:1, 0:cols]] + [srecv[s, 1:2, :] for s in (1, 2, 3)]
    highest = jnp.maximum(jnp.maximum(tops[0], tops[1]), jnp.maximum(tops[2], tops[3]))
    shares = [jnp.exp2(m - highest) for m in tops]
    whole = sum(s * w for s, w in zip(sums, shares))
    inverse = 1.0 / whole
    weights = [shares[0] * inverse] + [shares[s] * sums[s] * inverse for s in (1, 2, 3)]
    for j in range(length // 128):
        maps = []
        for m in range(2):
            at = slice(j * 256 + m * 128, j * 256 + (m + 1) * 128)
            value = acc[:, at] * weights[0][:, at]
            for s in (1, 2, 3):
                value = value + orecv[s, :, at].astype(F32) * weights[s][:, at]
            maps.append(value)
        mixed = maps[0] - lam_ref[0:1, :] * maps[1]
        spread = jnp.mean(mixed * mixed, axis=0, keepdims=True)
        normed = mixed * lax.rsqrt(spread + 1e-06)
        out_ref[j * 128 : (j + 1) * 128, :] = (normed.T * gain_ref[0:1, :] * 0.8).astype(BF16)

    for s in range(8):
        arrive(yb[s])
    for copy in started:
        copy.wait_send()
    own.wait()


def attention(q, k, v, gu, lam, gain):
    length = q.shape[0]
    cols = 2 * length
    dma = pltpu.SemaphoreType.DMA
    return pl.pallas_call(
        attention_kernel,
        name="attention",
        out_shape=(
            jax.ShapeDtypeStruct((length, VD), BF16),
            jax.ShapeDtypeStruct((NZ * NY, *gu.shape), BF16),
        ),
        in_specs=[VMEM] * 6,
        out_specs=(VMEM, ANY),
        scratch_shapes=[
            pltpu.VMEM((8, length, 128), BF16),
            pltpu.VMEM((8, length, 128), BF16),
            pltpu.VMEM((4, length, 128), BF16),
            pltpu.VMEM((2 * length, 256), BF16),
            pltpu.VMEM((2 * length, 128), BF16),
            pltpu.VMEM((256, 4 * cols), BF16),
            pltpu.VMEM((8, 4 * cols), F32),
            pltpu.VMEM((8, 4 * cols), F32),
            pltpu.VMEM((VD, 4 * cols), F32),
            pltpu.VMEM((4, VD, cols), BF16),
            pltpu.VMEM((4, 8, cols), F32),
            pltpu.VMEM((4, VD, cols), BF16),
            pltpu.VMEM((4, 8, cols), F32),
            dma((2, 4)),
            dma((8,)),
            dma((2, 4)),
            dma((8,)),
            dma((4,)),
            dma((4,)),
            dma((2, 4)),
            dma((2, 4)),
            dma((2, 8)),
            dma((2, 8)),
            dma((2, 8)),
            dma((2, 8)),
            dma((4,)),
            dma((4,)),
            dma((4,)),
            dma((4,)),
            dma,
        ],
        compiler_params=pltpu.CompilerParams(
            collective_id=0, has_side_effects=True, vmem_limit_bytes=60 * 2**20
        ),
    )(q, k, v, gu, lam, gain)


def tail_kernel(
    heads_ref,
    resid_ref,
    ow_ref,
    ng_ref,
    cw_ref,
    cb_ref,
    dw_ref,
    gug,
    out_ref,
    hall,
    nall,
    am,
    ssq,
    gu,
    big,
    gpad,
    gedge,
    halo,
    hid,
    dall,
    psib,
    rsib,
    pout,
    rout,
    xs,
    xr,
    cs,
    cr,
    ts,
    tr,
    es,
    er,
    ys,
    yrr,
    zs,
    zrr,
    bs,
    br,
    ps,
    pr,
    loc,
):
    sp, tp = lax.axis_index("sp"), lax.axis_index("tp")
    z, y = sp // NY, sp % NY
    x, c = tp // 2, tp % 2
    length = heads_ref.shape[0]
    half = length // 2
    width = resid_ref.shape[1]
    units = dw_ref.shape[1]
    hg = dw_ref.shape[0] // 2

    def xdev(dx, other=0):
        return (sp, ((x + dx) % 4) * 2 + (c + other) % 2)

    def index(dz, dy):
        return ((z + dz) % NZ) * NY + (y + dy) % NY

    def device(dz, dy):
        return (index(dz, dy), tp)

    xr_, xl_, sib = xdev(1), xdev(3), xdev(0, 1)
    zr, zl = device(1, 0), device(7, 0)
    after, before = ((sp + 1) % (NZ * NY), tp), ((sp + NZ * NY - 1) % (NZ * NY), tp)
    tp_peers = [(sp, (tp + i) % 8) for i in range(1, 8)]
    meet(tp_peers + [after, before, zr, zl] + [device(0, i) for i in (1, 2, 3)])
    started = []

    def go(copy):
        copy.start()
        started.append(copy)
        return copy

    def arrive(copies):
        for copy in copies:
            copy.wait_recv()

    load = pltpu.make_async_copy(gug, gu, loc)
    load.start()

    dy = [
        go(remote(dw_ref, dall.at[sp], ys.at[i], yrr.at[i], device(0, i))) for i in (1, 2, 3)
    ]
    dall[sp] = dw_ref[...]

    def dcol(dz):
        return pl.ds(((z + dz) % NZ) * NY, NY)

    def send_d(t):
        right, left = dcol(8 - t), dcol(t)
        if t == 3:
            right = pl.ds(((z + 8 - t) % NZ) * NY, NY // 2)
            left = pl.ds(((z + t) % NZ) * NY + NY // 2, NY // 2)
        return [
            go(remote(dall.at[right], dall.at[right], zs.at[0, t], zrr.at[0, t], zr)),
            go(remote(dall.at[left], dall.at[left], zs.at[1, t], zrr.at[1, t], zl)),
        ]

    def gather(stack, k):
        mine = stack.at[tp]
        one = [
            go(remote(mine, mine, xs.at[k, 0], xr.at[k, 0], xr_)),
            go(remote(mine, mine, xs.at[k, 1], xr.at[k, 1], xl_)),
        ]
        core = [go(remote(mine, mine, cs.at[k, 0], cr.at[k, 0], sib))]
        arrive(core)
        yield 0
        from_left = stack.at[((x + 3) % 4) * 2 + c]
        from_right = stack.at[((x + 1) % 4) * 2 + c]
        upper, lower = pl.ds(0, half), pl.ds(half, half)
        arrive(one[:1])
        two = [go(remote(from_left.at[upper], from_left.at[upper], xs.at[k, 2], xr.at[k, 2], xr_))]
        core.append(go(remote(from_left, from_left, cs.at[k, 1], cr.at[k, 1], sib)))
        arrive(one[1:])
        two.append(go(remote(from_right.at[lower], from_right.at[lower], xs.at[k, 3], xr.at[k, 3], xl_)))
        core.append(go(remote(from_right, from_right, cs.at[k, 2], cr.at[k, 2], sib)))
        arrive(core[1:2])
        yield 3
        arrive(core[2:3])
        yield 1
        far = stack.at[((x + 2) % 4) * 2 + c]
        arrive(two[:1])
        core.append(go(remote(far.at[upper], far.at[upper], cs.at[k, 3], cr.at[k, 3], sib)))
        arrive(two[1:])
        core.append(go(remote(far.at[lower], far.at[lower], cs.at[k, 4], cr.at[k, 4], sib)))
        arrive(core[3:5])
        yield 2

    hall[tp] = heads_ref[...]
    am[...] = resid_ref[...].astype(F32)
    for dx in gather(hall, 0):
        chip = (x + dx) % 4
        for core in range(2):
            rows = pl.ds(pl.multiple_of((chip * 2 + core) * VD, VD), VD)
            am[...] += jnp.dot(hall[chip * 2 + core], ow_ref[rows, :], preferred_element_type=F32)
    value = am[...]
    nall[tp] = (value * ng_ref[0:1, :]).astype(BF16)
    square = value * value
    square = square[:, 0:128] + square[:, 128:256]
    for j in range(length // 128):
        part = jnp.sum(square[j * 128 : (j + 1) * 128, :].T, axis=0, keepdims=True)
        ssq[tp, 0:8, j * 128 : (j + 1) * 128] = jnp.broadcast_to(part, (8, 128))

    arrive(dy)
    dz = [send_d(0)]
    load.wait()
    tiny = []

    def product(chip):
        a = jnp.concatenate([nall[chip * 2], nall[chip * 2 + 1]], axis=1)
        rows = pl.ds(pl.multiple_of(chip * 2 * width, 2 * width), 2 * width)
        return jnp.dot(a, gu[rows, :], preferred_element_type=F32)

    for n, dx in enumerate(gather(nall, 1)):
        if n == 0:
            tiny = [
                go(remote(ssq.at[tp], ssq.at[tp], ts.at[i - 1], tr.at[i - 1], (sp, (tp + i) % 8)))
                for i in range(1, 8)
            ]
            big[...] = product((x + dx) % 4)
        else:
            if n == 2:
                arrive(dz[0])
                dz.append(send_d(1))
            big[...] += product((x + dx) % 4)
    arrive(dz[1])
    dz.append(send_d(2))
    arrive(tiny)
    squares = sum(ssq[i, 0:1, :] for i in range(8))
    factor = lax.rsqrt(squares * (1.0 / D) + 1e-06)
    whole = units // 128 * 128
    rest = units - whole
    for j in range(length // 128):
        rows = slice(j * 128, (j + 1) * 128)
        column = jnp.broadcast_to(factor[:, rows], (128, 128)).T[:, 0:1]
        scaled = big[rows, :] * column
        gate = jnp.concatenate([scaled[:, 0:whole], scaled[:, 2 * whole : 2 * whole + rest]], axis=1)
        gpad[8 + j * 128 : 8 + (j + 1) * 128, :] = gate.astype(BF16).astype(F32)
        big[rows, whole:] = scaled[:, whole:]
    gedge[0] = gpad[8:24, :].astype(BF16)
    gedge[1] = gpad[8 + length - 16 : 8 + length, :].astype(BF16)
    edge = [
        go(remote(gedge.at[1], halo.at[0], es.at[0], er.at[0], after)),
        go(remote(gedge.at[0], halo.at[1], es.at[1], er.at[1], before)),
    ]
    arrive(edge)
    previous = jnp.where(sp == 0, 0.0, halo[0].astype(F32)[15:16, :])
    following = jnp.where(sp == NZ * NY - 1, 0.0, halo[1].astype(F32)[0:1, :])
    gpad[7:8, :] = previous
    gpad[8 + length : 9 + length, :] = following
    for j in range(length // 128):
        rows = slice(j * 128, (j + 1) * 128)
        at = 8 + j * 128
        conv = (
            gpad[at - 1 : at + 127, :] * cw_ref[0:1, :]
            + gpad[at : at + 128, :] * cw_ref[1:2, :]
            + gpad[at + 1 : at + 129, :] * cw_ref[2:3, :]
            + cb_ref[0:1, :]
        )
        up = jnp.concatenate([big[rows, whole : 2 * whole], big[rows, 2 * whole + rest :]], axis=1)
        hid[rows, :] = (conv / (1.0 + jnp.exp(-conv)) * up).astype(BF16)

    arrive(dz[2])
    dz.append(send_d(3))
    arrive(dz[3])
    per = width // dw_ref.shape[0]

    def down(target):
        w = dall[pl.ds(target * per, per)].reshape(width, units)
        return lax.dot_general(
            hid[...], w, (((1,), (1,)), ((), ())), preferred_element_type=F32
        )

    order = (2, 1, 3, 0)
    for dx in order:
        psib[dx] = down(((x + dx) % 4) * 2 + (1 - c)).astype(BF16)
        go(remote(psib.at[dx], rsib.at[dx], bs.at[dx], br.at[dx], sib))
    final = []
    for dx in order:
        piece = down(((x + dx) % 4) * 2 + c)
        remote(psib.at[dx], rsib.at[dx], bs.at[dx], br.at[dx], sib).wait_recv()
        piece = piece + rsib[dx].astype(F32)
        if dx == 0:
            am[...] += piece
        else:
            pout[dx] = piece.astype(BF16)
            final.append(go(remote(pout.at[dx], rout.at[dx], ps.at[dx], pr.at[dx], xdev(dx))))
    arrive(final)
    out_ref[...] = (
        am[...] + (rout[1].astype(F32) + rout[2].astype(F32) + rout[3].astype(F32))
    ).astype(BF16)
    for copy in started:
        copy.wait_send()


def tail(heads, resid, ow, ng, cw, cb, dw, gug):
    length, width = resid.shape
    units = dw.shape[1]
    dma = pltpu.SemaphoreType.DMA
    return pl.pallas_call(
        tail_kernel,
        name="tail",
        out_shape=jax.ShapeDtypeStruct((length, width), BF16),
        in_specs=[VMEM] * 7 + [ANY],
        out_specs=VMEM,
        scratch_shapes=[
            pltpu.VMEM((8, length, VD), BF16),
            pltpu.VMEM((8, length, width), BF16),
            pltpu.VMEM((length, width), F32),
            pltpu.VMEM((8, 8, length), F32),
            pltpu.VMEM(gug.shape, BF16),
            pltpu.VMEM((length, 2 * units), F32),
            pltpu.VMEM((length + 16, units), F32),
            pltpu.VMEM((2, 16, units), BF16),
            pltpu.VMEM((2, 16, units), BF16),
            pltpu.VMEM((length, units), BF16),
            pltpu.VMEM((NZ * NY, *dw.shape), BF16),
            pltpu.VMEM((4, length, width), BF16),
            pltpu.VMEM((4, length, width), BF16),
            pltpu.VMEM((4, length, width), BF16),
            pltpu.VMEM((4, length, width), BF16),
            dma((2, 4)),
            dma((2, 4)),
            dma((2, 5)),
            dma((2, 5)),
            dma((7,)),
            dma((7,)),
            dma((2,)),
            dma((2,)),
            dma((4,)),
            dma((4,)),
            dma((2, 4)),
            dma((2, 4)),
            dma((4,)),
            dma((4,)),
            dma((4,)),
            dma((4,)),
            dma,
        ],
        compiler_params=pltpu.CompilerParams(
            collective_id=1, has_side_effects=True, vmem_limit_bytes=60 * 2**20
        ),
    )(heads, resid, ow, ng, cw, cb, dw, gug)


def on_device(
    resid,
    queries,
    keys,
    values,
    mix_lambda,
    head_gain,
    out_weight,
    norm_gain,
    gate_weight,
    up_weight,
    conv_weight,
    conv_bias,
    down_weight,
):
    units = gate_weight.shape[1]
    whole = units // 128 * 128
    gu = jnp.concatenate(
        [gate_weight[:, :whole], up_weight[:, :whole], gate_weight[:, whole:], up_weight[:, whole:]], axis=1
    )
    lam = jnp.broadcast_to(mix_lambda.reshape(1, 1), (8, 128))
    gain = jnp.broadcast_to(head_gain[None, :], (8, VD))
    heads_out, gug = attention(queries, keys, values, gu, lam, gain)
    return tail(
        heads_out,
        resid,
        out_weight,
        norm_gain[None, :],
        conv_weight,
        conv_bias[None, :],
        down_weight.T,
        gug.reshape(-1, gug.shape[-1]),
    )


def solution(mesh):
    return jax.shard_map(
        on_device,
        mesh=mesh,
        in_specs=(
            P("sp", "tp"),
            P("sp", "tp"),
            P("sp", "tp"),
            P("sp", "tp"),
            P("tp"),
            P(),
            P(None, "tp"),
            P("tp"),
            P("sp", "tp"),
            P("sp", "tp"),
            P(None, "tp"),
            P("tp"),
            P("tp", "sp"),
        ),
        out_specs=P("sp", "tp"),
        check_vma=False,
    )
```

```python
import functools

import jax
import jax.numpy as jnp
from jax import lax
from jax.experimental import pallas as pl
from jax.experimental.pallas import tpu as pltpu
from jax.sharding import PartitionSpec as P

D = 2048
HD = 64
VD = 128
LOG2E = 1.4426950408889634
NZ = 8
NY = 4
F32 = jnp.float32
BF16 = jnp.bfloat16
MESH = pl.DeviceIdType.MESH
VMEM = pl.BlockSpec(memory_space=pltpu.VMEM)
ANY = pl.BlockSpec(memory_space=pl.ANY)
SMEM = pl.BlockSpec(memory_space=pltpu.SMEM)


def remote(src, dst, send, recv, device):
    return pltpu.make_async_remote_copy(
        src_ref=src, dst_ref=dst, send_sem=send, recv_sem=recv, device_id=device, device_id_type=MESH
    )


def meet(peers):
    barrier = pltpu.get_barrier_semaphore()
    for peer in peers:
        pl.semaphore_signal(barrier, inc=1, device_id=peer, device_id_type=MESH)
    pl.semaphore_wait(barrier, len(peers))


def attention_kernel(
    q_ref,
    k_ref,
    v_ref,
    gate_ref,
    up_ref,
    lam_ref,
    gain_ref,
    out_ref,
    gug,
    guo,
    kbuf,
    vbuf,
    qbuf,
    kk,
    vv,
    qbd,
    top,
    total,
    acc,
    lse,
    part,
    relay,
    landed,
    ks,
    kr,
    vs,
    vr,
    qs,
    qr,
    gs,
    gr,
    ya_s,
    ya_r,
    yb_s,
    yb_r,
    hs,
    hr,
    hz_s,
    hz_r,
    ls,
    lr,
    ms,
    mr,
    loc,
):
    sp, tp = lax.axis_index("sp"), lax.axis_index("tp")
    z, y = sp // NY, sp % NY
    length = q_ref.shape[0]
    cols = 2 * length
    half = length // 2
    units = gate_ref.shape[1]
    whole = units // 128 * 128
    rest = units - whole
    first = pl.ds(0, 48)
    last = pl.ds(48, 16)

    def index(dz, dy):
        return ((z + dz) % NZ) * NY + (y + dy) % NY

    def device(dz, dy):
        return (index(dz, dy), tp)

    zr, zl = device(1, 0), device(7, 0)
    yr, yl = device(0, 1), device(0, 3)
    guo[:, 0:whole] = gate_ref[:, 0:whole]
    guo[:, whole : 2 * whole] = up_ref[:, 0:whole]
    guo[:, 2 * whole :] = jnp.concatenate([gate_ref[:, whole:], up_ref[:, whole:]], axis=1)
    meet([zr, zl, yr, yl, device(0, 2)])
    started = []

    def go(copy):
        copy.start()
        started.append(copy)
        return copy

    def arrive(copies):
        for copy in copies:
            copy.wait_recv()

    def kslot(s):
        return k_ref if s == 0 else kbuf.at[s]

    def vslot(s):
        return v_ref if s == 0 else vbuf.at[s]

    def send_kv(t):
        right, left = t, (8 - t) % 8
        out = [go(remote(kslot(right), kbuf.at[t + 1], ks.at[0, t], kr.at[t + 1], zr))]
        if t < 3:
            out.append(go(remote(kslot(left), kbuf.at[7 - t], ks.at[1, t], kr.at[7 - t], zl)))
            out.append(go(remote(vslot(right), vbuf.at[t + 1], vs.at[0, t], vr.at[t + 1], zr)))
        out.append(go(remote(vslot(left), vbuf.at[7 - t], vs.at[1, t], vr.at[7 - t], zl)))
        return out

    def source(s, rows):
        return guo.at[rows] if s == 0 else gug.at[index(8 - s, 0), rows]

    def parts(s):
        return (pl.ds(0, 16), pl.ds(16, 32)) if s % 2 == 0 else (pl.ds(0, 32), pl.ds(32, 16))

    def send_g(t):
        right, left = t, (8 - t) % 8
        rows_r, rows_l = parts(0) if t == 3 else (first, first)
        return [
            go(remote(source(right, rows_r), gug.at[index(8 - right, 0), rows_r], gs.at[0, t], gr.at[0, t], zr)),
            go(remote(source(left, rows_l), gug.at[index(8 - left, 0), rows_l], gs.at[1, t], gr.at[1, t], zl)),
        ]

    def send_ya(s):
        dst = gug.at[index(8 - s, 0), first]
        return [
            go(remote(source(s, first), dst, ya_s.at[0, s], ya_r.at[0, s], yr)),
            go(remote(source(s, first), dst, ya_s.at[1, s], ya_r.at[1, s], yl)),
        ]

    def send_yb(s):
        rows_r, rows_l = parts(s)
        a = gug.at[index(8 - s, 3), rows_r]
        b = gug.at[index(8 - s, 1), rows_l]
        return [
            go(remote(a, a, yb_s.at[0, s], yb_r.at[0, s], yr)),
            go(remote(b, b, yb_s.at[1, s], yb_r.at[1, s], yl)),
        ]

    def send_h(t):
        right, left = ((z + 8 - t) % NZ) * NY, ((z + t) % NZ) * NY
        if t < 3:
            a, b = gug.at[pl.ds(right, NY), last], gug.at[pl.ds(left, NY), last]
        else:
            a, b = gug.at[pl.ds(right, 2), last], gug.at[pl.ds(left + 2, 2), last]
        return [
            go(remote(a, a, hz_s.at[0, t], hz_r.at[0, t], zr)),
            go(remote(b, b, hz_s.at[1, t], hz_r.at[1, t], zl)),
        ]

    qa = [
        go(remote(q_ref, qbuf.at[1], qs.at[0], qr.at[0], yr)),
        go(remote(q_ref, qbuf.at[3], qs.at[1], qr.at[1], yl)),
    ]
    kv = [send_kv(0)]
    own = pltpu.make_async_copy(guo, gug.at[sp], loc)
    own.start()
    g = [send_g(0)]
    hy = [
        go(remote(guo.at[last], gug.at[sp, last], hs.at[i - 1], hr.at[i - 1], device(0, i)))
        for i in (1, 3, 2)
    ]
    ya = {0: send_ya(0)}
    yb = {}
    h = []

    top[...] = jnp.full(top.shape, -1e30, F32)
    total[...] = jnp.zeros(total.shape, F32)
    acc[...] = jnp.zeros(acc.shape, F32)
    row = lax.broadcasted_iota(jnp.int32, (2 * HD, 128), 0)

    def lay_queries(src, slot):
        for j in range(length // 128):
            turned = src[j * 128 : (j + 1) * 128, :].astype(F32).T * (LOG2E * HD**-0.5)
            for m in range(2):
                at = slot * cols + j * 256 + m * 128
                kept = jnp.where((row < HD) if m == 0 else (row >= HD), turned, 0.0)
                high = kept.astype(BF16)
                qbd[0:128, at : at + 128] = high
                qbd[128:256, at : at + 128] = (kept - high.astype(F32)).astype(BF16)

    def stage(slots):
        for n, s in enumerate(slots):
            kb = kslot(s)[...]
            kk[n * length : (n + 1) * length, 0:128] = kb
            kk[n * length : (n + 1) * length, 128:256] = kb
            vv[n * length : (n + 1) * length, :] = vslot(s)[...]

    def attend(count, begin, end):
        keys = count * length

        def tile(i, carry):
            at = pl.ds(pl.multiple_of(i * cols, cols), cols)
            scores = jnp.dot(kk[0:keys, :], qbd[:, at], preferred_element_type=F32)
            before = top[0:1, at]
            now = jnp.maximum(before, jnp.max(scores, axis=0, keepdims=True))
            shifted = jnp.exp2(scores - now)
            factor = jnp.exp2(before - now)
            top[0:1, at] = now
            total[0:1, at] = total[0:1, at] * factor + jnp.sum(shifted, axis=0, keepdims=True)
            acc[:, at] = acc[:, at] * factor + lax.dot_general(
                vv[0:keys, :],
                shifted.astype(BF16),
                (((0,), (0,)), ((), ())),
                preferred_element_type=F32,
            )
            return carry

        lax.fori_loop(begin, end, tile, 0)

    lay_queries(q_ref, 0)
    stage([0])
    attend(1, 0, 1)
    arrive(qa)
    low, high_rows = pl.ds(0, half), pl.ds(half, half)
    qb = [
        go(remote(qbuf.at[1, low], qbuf.at[2, low], qs.at[2], qr.at[2], yr)),
        go(remote(qbuf.at[3, high_rows], qbuf.at[2, high_rows], qs.at[3], qr.at[3], yl)),
    ]
    lay_queries(qbuf.at[1], 1)
    lay_queries(qbuf.at[3], 3)
    attend(1, 1, 2)
    attend(1, 3, 4)
    arrive(qb)
    lay_queries(qbuf.at[2], 2)
    attend(1, 2, 3)

    for t in range(1, 5):
        arrive(kv[t - 1])
        if t < 4:
            kv.append(send_kv(t))
        arrive(g[t - 1])
        if t < 4:
            g.append(send_g(t))
        if t == 2:
            arrive(hy)
            own.wait()
            h.append(send_h(0))
        elif t > 2:
            arrive(h[t - 3])
            h.append(send_h(t - 2))
        slots = [t, 8 - t] if t < 4 else [4]
        for s in slots:
            ya[s] = send_ya(s)
        for s in (0,) if t == 1 else (t - 1, 9 - t):
            arrive(ya[s])
            yb[s] = send_yb(s)
        stage(slots)
        attend(len(slots), 0, 4)

    for slot in range(4):
        for n in range(2):
            at = slice(slot * cols + n * length, slot * cols + (n + 1) * length)
            lse[0, 2 * slot + n : 2 * slot + n + 1, :] = top[0:1, at] + jnp.log2(total[0:1, at])
    stats = [
        go(remote(lse.at[0], lse.at[4 - i], ls.at[i - 1], lr.at[3 - i], device(0, i))) for i in (2, 1, 3)
    ]
    arrive(h[2])
    h.append(send_h(3))
    arrive(ya[4])
    yb[4] = send_yb(4)
    arrive(stats)
    weights = {}
    for slot in range(4):
        for n in range(2):
            logs = []
            for e in range(4):
                r = 2 * ((slot + e) % 4) + n
                logs.append(lse[e, r : r + 1, :])
            highest = jnp.maximum(jnp.maximum(logs[0], logs[1]), jnp.maximum(logs[2], logs[3]))
            shares = [jnp.exp2(v - highest) for v in logs]
            at = slice(slot * cols + n * length, slot * cols + (n + 1) * length)
            weights[slot, n] = shares[0] / ((shares[0] + shares[1] + shares[2] + shares[3]) * total[0:1, at])

    def mixture(slot, rows):
        out = []
        for j in range(length // 128):
            maps = []
            for m in range(2):
                at = j * 256 + m * 128
                w = weights[slot, at // length][:, at % length : at % length + 128]
                maps.append(acc[rows, slot * cols + at : slot * cols + at + 128] * w)
            out.append(maps[0] - lam_ref[0] * maps[1])
        return jnp.concatenate(out, axis=1)

    up_rows, low_rows = slice(0, 64), slice(64, 128)
    at_up, at_low = pl.ds(0, 64), pl.ds(64, 64)
    part[2, up_rows, :] = mixture(2, up_rows).astype(BF16)
    part[2, low_rows, :] = mixture(2, low_rows).astype(BF16)
    over = [
        go(remote(part.at[2, at_up], relay.at[0], ms.at[0], mr.at[0], yr)),
        go(remote(part.at[2, at_low], relay.at[1], ms.at[1], mr.at[1], yl)),
    ]
    part[3, low_rows, :] = mixture(3, low_rows).astype(BF16)
    part[1, up_rows, :] = mixture(1, up_rows).astype(BF16)
    ends = [
        go(remote(part.at[3, at_low], landed.at[0, at_low], ms.at[2], mr.at[2], yr)),
        go(remote(part.at[1, at_up], landed.at[1, at_up], ms.at[3], mr.at[3], yl)),
    ]
    third, firsts = mixture(3, up_rows), mixture(1, low_rows)
    arrive(over)
    part[3, up_rows, :] = (third + relay[0].astype(F32)).astype(BF16)
    part[1, low_rows, :] = (firsts + relay[1].astype(F32)).astype(BF16)
    ends += [
        go(remote(part.at[3, at_up], landed.at[0, at_up], ms.at[4], mr.at[4], yr)),
        go(remote(part.at[1, at_low], landed.at[1, at_low], ms.at[5], mr.at[5], yl)),
    ]
    mixed = mixture(0, slice(0, 128))
    arrive(ends)
    mixed = mixed + (landed[0].astype(F32) + landed[1].astype(F32))
    spread = jnp.mean(mixed * mixed, axis=0, keepdims=True)
    normed = mixed * lax.rsqrt(spread + 1e-06)
    gain = gain_ref[...][None, :] * 0.8
    for j in range(length // 128):
        at = slice(j * 128, (j + 1) * 128)
        out_ref[at, :] = (normed[:, at].T * gain).astype(BF16)

    for s in range(8):
        arrive(yb[s])
    arrive(h[3])
    for copy in started:
        copy.wait_send()


def attention(q, k, v, gate, up, lam, gain):
    length = q.shape[0]
    cols = 2 * length
    dma = pltpu.SemaphoreType.DMA
    rows, units = gate.shape
    return pl.pallas_call(
        attention_kernel,
        name="attention",
        out_shape=(
            jax.ShapeDtypeStruct((length, VD), BF16),
            jax.ShapeDtypeStruct((NZ * NY, rows, 2 * units), BF16),
        ),
        in_specs=[VMEM] * 5 + [SMEM, VMEM],
        out_specs=(VMEM, ANY),
        scratch_shapes=[
            pltpu.VMEM((rows, 2 * units), BF16),
            pltpu.VMEM((8, length, 128), BF16),
            pltpu.VMEM((8, length, 128), BF16),
            pltpu.VMEM((4, length, 128), BF16),
            pltpu.VMEM((2 * length, 256), BF16),
            pltpu.VMEM((2 * length, 128), BF16),
            pltpu.VMEM((256, 4 * cols), BF16),
            pltpu.VMEM((8, 4 * cols), F32),
            pltpu.VMEM((8, 4 * cols), F32),
            pltpu.VMEM((VD, 4 * cols), F32),
            pltpu.VMEM((4, 8, length), F32),
            pltpu.VMEM((4, VD, length), BF16),
            pltpu.VMEM((2, VD // 2, length), BF16),
            pltpu.VMEM((2, VD, length), BF16),
            dma((2, 4)),
            dma((8,)),
            dma((2, 4)),
            dma((8,)),
            dma((4,)),
            dma((4,)),
            dma((2, 4)),
            dma((2, 4)),
            dma((2, 8)),
            dma((2, 8)),
            dma((2, 8)),
            dma((2, 8)),
            dma((3,)),
            dma((3,)),
            dma((2, 4)),
            dma((2, 4)),
            dma((3,)),
            dma((3,)),
            dma((6,)),
            dma((6,)),
            dma,
        ],
        compiler_params=pltpu.CompilerParams(
            collective_id=0, has_side_effects=True, vmem_limit_bytes=60 * 2**20
        ),
    )(q, k, v, gate, up, lam, gain)


def tail_kernel(
    heads_ref,
    resid_ref,
    ow_ref,
    ng_ref,
    cw_ref,
    cb_ref,
    dw_ref,
    gug,
    out_ref,
    hall,
    nall,
    am,
    ssq,
    gu,
    big,
    gpad,
    gedge,
    halo,
    hid,
    dall,
    psib,
    rsib,
    pout,
    relayed,
    rout,
    keep,
    xs,
    xr,
    cs,
    cr,
    ts,
    tr,
    es,
    er,
    ys,
    yrr,
    zs,
    zrr,
    as_,
    ar,
    ya_s,
    ya_r,
    yb_s,
    yb_r,
    bs,
    br,
    ps,
    pr,
    loc,
):
    sp, tp = lax.axis_index("sp"), lax.axis_index("tp")
    z, y = sp // NY, sp % NY
    x, c = tp // 2, tp % 2
    length = heads_ref.shape[0]
    half = length // 2
    width = resid_ref.shape[1]
    units = dw_ref.shape[1]
    units_rows = dw_ref.shape[0]

    def xdev(dx, other=0):
        return (sp, ((x + dx) % 4) * 2 + (c + other) % 2)

    def index(dz, dy):
        return ((z + dz) % NZ) * NY + (y + dy) % NY

    def device(dz, dy):
        return (index(dz, dy), tp)

    xr_, xl_, sib = xdev(1), xdev(3), xdev(0, 1)
    zr, zl = device(1, 0), device(7, 0)
    yr, yl = device(0, 1), device(0, 3)
    hall[tp] = heads_ref[...]
    dall[sp] = dw_ref[...]
    after, before = ((sp + 1) % (NZ * NY), tp), ((sp + NZ * NY - 1) % (NZ * NY), tp)
    tp_peers = [(sp, (tp + i) % 8) for i in range(1, 8)]
    meet(tp_peers + [after, before, zr, zl] + [device(0, i) for i in (1, 2, 3)])
    started = []

    def go(copy):
        copy.start()
        started.append(copy)
        return copy

    def arrive(copies):
        for copy in copies:
            copy.wait_recv()

    load = pltpu.make_async_copy(gug, gu, loc)
    load.start()
    turn = units_rows // 2
    early, late = pl.ds(0, turn), pl.ds(turn, turn)
    upper_q, lower_q = pl.ds(0, turn // 2), pl.ds(turn // 2, turn // 2)

    def source(s, rows):
        return dw_ref.at[rows] if s == 0 else dall.at[index(8 - s, 0), rows]

    def send_a(t):
        right, left = t, (8 - t) % 8
        rows_r, rows_l = (upper_q, lower_q) if t == 3 else (early, early)
        return [
            go(remote(source(right, rows_r), dall.at[index(8 - right, 0), rows_r], as_.at[0, t], ar.at[0, t], zr)),
            go(remote(source(left, rows_l), dall.at[index(8 - left, 0), rows_l], as_.at[1, t], ar.at[1, t], zl)),
        ]

    def send_ya(s):
        dst = dall.at[index(8 - s, 0), early]
        return [
            go(remote(source(s, early), dst, ya_s.at[0, s], ya_r.at[0, s], yr)),
            go(remote(source(s, early), dst, ya_s.at[1, s], ya_r.at[1, s], yl)),
        ]

    def send_yb(s):
        a = dall.at[index(8 - s, 3), upper_q]
        b = dall.at[index(8 - s, 1), lower_q]
        return [
            go(remote(a, a, yb_s.at[0, s], yb_r.at[0, s], yr)),
            go(remote(b, b, yb_s.at[1, s], yb_r.at[1, s], yl)),
        ]

    def send_d(t):
        right, left = ((z + 8 - t) % NZ) * NY, ((z + t) % NZ) * NY
        if t < 3:
            a, b = dall.at[pl.ds(right, NY), late], dall.at[pl.ds(left, NY), late]
        else:
            a, b = dall.at[pl.ds(right, 2), late], dall.at[pl.ds(left + 2, 2), late]
        return [
            go(remote(a, a, zs.at[0, t], zrr.at[0, t], zr)),
            go(remote(b, b, zs.at[1, t], zrr.at[1, t], zl)),
        ]

    def gather(stack, k):
        mine = stack.at[tp]
        one = [
            go(remote(mine, mine, xs.at[k, 0], xr.at[k, 0], xr_)),
            go(remote(mine, mine, xs.at[k, 1], xr.at[k, 1], xl_)),
        ]
        core = [go(remote(mine, mine, cs.at[k, 0], cr.at[k, 0], sib))]
        yield None
        arrive(core)
        yield 0
        from_left = stack.at[((x + 3) % 4) * 2 + c]
        from_right = stack.at[((x + 1) % 4) * 2 + c]
        upper, lower = pl.ds(0, half), pl.ds(half, half)
        arrive(one[:1])
        two = [go(remote(from_left.at[upper], from_left.at[upper], xs.at[k, 2], xr.at[k, 2], xr_))]
        core.append(go(remote(from_left, from_left, cs.at[k, 1], cr.at[k, 1], sib)))
        arrive(one[1:])
        two.append(go(remote(from_right.at[lower], from_right.at[lower], xs.at[k, 3], xr.at[k, 3], xl_)))
        core.append(go(remote(from_right, from_right, cs.at[k, 2], cr.at[k, 2], sib)))
        arrive(core[1:2])
        yield 3
        arrive(core[2:3])
        yield 1
        far = stack.at[((x + 2) % 4) * 2 + c]
        arrive(two[:1])
        core.append(go(remote(far.at[upper], far.at[upper], cs.at[k, 3], cr.at[k, 3], sib)))
        arrive(two[1:])
        core.append(go(remote(far.at[lower], far.at[lower], cs.at[k, 4], cr.at[k, 4], sib)))
        arrive(core[3:5])
        yield 2

    heads = gather(hall, 0)
    next(heads)
    da = [send_a(0)]
    along = [
        go(remote(dw_ref.at[late], dall.at[sp, late], ys.at[i - 1], yrr.at[i - 1], device(0, i)))
        for i in (1, 3, 2)
    ]
    ya, yb, dz = {0: send_ya(0)}, {}, []
    am[...] = resid_ref[...].astype(F32)

    def relay_a(t):
        arrive(da[t])
        if t < 3:
            da.append(send_a(t + 1))
        for s in (t + 1, 7 - t) if t < 3 else (4,):
            ya[s] = send_ya(s)

    def relay_y(*slots):
        for s in slots:
            arrive(ya[s])
            yb[s] = send_yb(s)

    def relay_d(t):
        arrive(along if t == 0 else dz[t - 1])
        dz.append(send_d(t))

    for n, dx in enumerate(heads):
        chip = (x + dx) % 4
        for core in range(2):
            rows = pl.ds(pl.multiple_of((chip * 2 + core) * VD, VD), VD)
            am[...] += jnp.dot(hall[chip * 2 + core], ow_ref[rows, :], preferred_element_type=F32)
        if n == 0:
            relay_a(0)
            relay_d(0)
            relay_y(0)
        elif n == 2:
            relay_a(1)
            relay_y(1, 7)
    value = am[...]
    nall[tp] = (value * ng_ref[...][None, :]).astype(BF16)
    rows_in = gather(nall, 1)
    next(rows_in)
    square = value * value
    square = square[:, 0:128] + square[:, 128:256]
    for j in range(length // 128):
        ssq[tp, j : j + 1, :] = jnp.sum(square[j * 128 : (j + 1) * 128, :].T, axis=0, keepdims=True)
    ssq[tp, length // 128 :, :] = jnp.zeros((8 - length // 128, 128), F32)
    tiny = [
        go(remote(ssq.at[tp], ssq.at[tp], ts.at[i - 1], tr.at[i - 1], (sp, (tp + i) % 8)))
        for i in range(1, 8)
    ]
    relay_a(2)
    relay_y(2, 6)
    relay_d(1)
    load.wait()

    def product(chip):
        a = jnp.concatenate([nall[chip * 2], nall[chip * 2 + 1]], axis=1)
        rows = pl.ds(pl.multiple_of(chip * 2 * width, 2 * width), 2 * width)
        return jnp.dot(a, gu[rows, :], preferred_element_type=F32)

    for n, dx in enumerate(rows_in):
        if n == 0:
            big[...] = product((x + dx) % 4)
            relay_a(3)
            relay_y(3, 5)
        else:
            big[...] += product((x + dx) % 4)
        if n == 2:
            relay_d(2)
            relay_y(4)
    relay_d(3)
    arrive(tiny)
    squares = ssq[0]
    for i in range(1, 8):
        squares = squares + ssq[i]
    factor = lax.rsqrt(squares * (1.0 / D) + 1e-06)
    whole = units // 128 * 128
    rest = units - whole
    for j in range(length // 128):
        rows = slice(j * 128, (j + 1) * 128)
        column = jnp.broadcast_to(factor[j : j + 1, :], (128, 128)).T[:, 0:1]
        scaled = big[rows, :] * column
        gate = jnp.concatenate([scaled[:, 0:whole], scaled[:, 2 * whole : 2 * whole + rest]], axis=1)
        gpad[8 + j * 128 : 8 + (j + 1) * 128, :] = gate.astype(BF16).astype(F32)
        big[rows, whole:] = scaled[:, whole:]
    gedge[0] = gpad[8:24, :].astype(BF16)
    gedge[1] = gpad[8 + length - 16 : 8 + length, :].astype(BF16)
    edge = [
        go(remote(gedge.at[1], halo.at[0], es.at[0], er.at[0], after)),
        go(remote(gedge.at[0], halo.at[1], es.at[1], er.at[1], before)),
    ]
    arrive(edge)
    previous = jnp.where(sp == 0, 0.0, halo[0].astype(F32)[15:16, :])
    following = jnp.where(sp == NZ * NY - 1, 0.0, halo[1].astype(F32)[0:1, :])
    gpad[7:8, :] = previous
    gpad[8 + length : 9 + length, :] = following
    for j in range(length // 128):
        rows = slice(j * 128, (j + 1) * 128)
        at = 8 + j * 128
        conv = (
            gpad[at - 1 : at + 127, :] * cw_ref[0:1, :]
            + gpad[at : at + 128, :] * cw_ref[1:2, :]
            + gpad[at + 1 : at + 129, :] * cw_ref[2:3, :]
            + cb_ref[...][None, :]
        )
        up = jnp.concatenate([big[rows, whole : 2 * whole], big[rows, 2 * whole + rest :]], axis=1)
        hid[rows, :] = (conv / (1.0 + jnp.exp(-conv)) * up).astype(BF16)

    for s in range(8):
        arrive(yb[s])
    arrive(dz[3])
    per = width // units_rows

    def down(target):
        w = dall[pl.ds(target * per, per)].reshape(width, units)
        return lax.dot_general(
            hid[...], w, (((1,), (1,)), ((), ())), preferred_element_type=F32
        )

    order = (2, 1, 3, 0)
    crossing = {}
    for dx in order:
        psib[dx] = down(((x + dx) % 4) * 2 + (1 - c)).astype(BF16)
        crossing[dx] = go(remote(psib.at[dx], rsib.at[dx], bs.at[dx], br.at[dx], sib))
    upper, lower = slice(0, half), slice(half, length)
    at_upper, at_lower = pl.ds(0, half), pl.ds(half, half)
    ends = []
    for dx in order:
        piece = down(((x + dx) % 4) * 2 + c)
        arrive([crossing[dx]])
        piece = piece + rsib[dx].astype(F32)
        if dx == 2:
            pout[2] = piece.astype(BF16)
            over = [
                go(remote(pout.at[2, at_upper], relayed.at[0], ps.at[0], pr.at[0], xr_)),
                go(remote(pout.at[2, at_lower], relayed.at[1], ps.at[1], pr.at[1], xl_)),
            ]
        elif dx == 1:
            pout[1, lower, :] = piece[lower, :].astype(BF16)
            ends.append(go(remote(pout.at[1, at_lower], rout.at[0, at_lower], ps.at[2], pr.at[2], xr_)))
            keep[0] = piece[upper, :]
        elif dx == 3:
            pout[3, upper, :] = piece[upper, :].astype(BF16)
            ends.append(go(remote(pout.at[3, at_upper], rout.at[1, at_upper], ps.at[3], pr.at[3], xl_)))
            keep[1] = piece[lower, :]
            arrive(over)
            pout[1, upper, :] = (keep[0] + relayed[0].astype(F32)).astype(BF16)
            ends.append(go(remote(pout.at[1, at_upper], rout.at[0, at_upper], ps.at[4], pr.at[4], xr_)))
            pout[3, lower, :] = (keep[1] + relayed[1].astype(F32)).astype(BF16)
            ends.append(go(remote(pout.at[3, at_lower], rout.at[1, at_lower], ps.at[5], pr.at[5], xl_)))
        else:
            am[...] += piece
    arrive(ends)
    out_ref[...] = (am[...] + (rout[0].astype(F32) + rout[1].astype(F32))).astype(BF16)
    for copy in started:
        copy.wait_send()


def tail(heads, resid, ow, ng, cw, cb, dw, gug):
    length, width = resid.shape
    units = dw.shape[1]
    dma = pltpu.SemaphoreType.DMA
    return pl.pallas_call(
        tail_kernel,
        name="tail",
        out_shape=jax.ShapeDtypeStruct((length, width), BF16),
        in_specs=[VMEM] * 7 + [ANY],
        out_specs=VMEM,
        scratch_shapes=[
            pltpu.VMEM((8, length, VD), BF16),
            pltpu.VMEM((8, length, width), BF16),
            pltpu.VMEM((length, width), F32),
            pltpu.VMEM((8, 8, 128), F32),
            pltpu.VMEM(gug.shape, BF16),
            pltpu.VMEM((length, 2 * units), F32),
            pltpu.VMEM((length + 16, units), F32),
            pltpu.VMEM((2, 16, units), BF16),
            pltpu.VMEM((2, 16, units), BF16),
            pltpu.VMEM((length, units), BF16),
            pltpu.VMEM((NZ * NY, *dw.shape), BF16),
            pltpu.VMEM((4, length, width), BF16),
            pltpu.VMEM((4, length, width), BF16),
            pltpu.VMEM((4, length, width), BF16),
            pltpu.VMEM((2, length // 2, width), BF16),
            pltpu.VMEM((2, length, width), BF16),
            pltpu.VMEM((2, length // 2, width), F32),
            dma((2, 4)),
            dma((2, 4)),
            dma((2, 5)),
            dma((2, 5)),
            dma((7,)),
            dma((7,)),
            dma((2,)),
            dma((2,)),
            dma((3,)),
            dma((3,)),
            dma((2, 4)),
            dma((2, 4)),
            dma((2, 4)),
            dma((2, 4)),
            dma((2, 8)),
            dma((2, 8)),
            dma((2, 8)),
            dma((2, 8)),
            dma((4,)),
            dma((4,)),
            dma((6,)),
            dma((6,)),
            dma,
        ],
        compiler_params=pltpu.CompilerParams(
            collective_id=1, has_side_effects=True, vmem_limit_bytes=60 * 2**20
        ),
    )(heads, resid, ow, ng, cw, cb, dw, gug)


def on_device(
    resid,
    queries,
    keys,
    values,
    mix_lambda,
    head_gain,
    out_weight,
    norm_gain,
    gate_weight,
    up_weight,
    conv_weight,
    conv_bias,
    down_weight,
):
    heads_out, gug = attention(queries, keys, values, gate_weight, up_weight, mix_lambda, head_gain)
    return tail(
        heads_out,
        resid,
        out_weight,
        norm_gain,
        conv_weight,
        conv_bias,
        down_weight.T,
        gug.reshape(-1, gug.shape[-1]),
    )


def solution(mesh):
    return jax.shard_map(
        on_device,
        mesh=mesh,
        in_specs=(
            P("sp", "tp"),
            P("sp", "tp"),
            P("sp", "tp"),
            P("sp", "tp"),
            P("tp"),
            P(),
            P(None, "tp"),
            P("tp"),
            P("sp", "tp"),
            P("sp", "tp"),
            P(None, "tp"),
            P("tp"),
            P("tp", "sp"),
        ),
        out_specs=P("sp", "tp"),
        check_vma=False,
    )
```

```python
import jax
import jax.numpy as jnp
from jax import lax
from jax.experimental import pallas as pl
from jax.experimental.pallas import tpu as pltpu
from jax.sharding import PartitionSpec as P

D = 2048
HD = 64
VD = 128
LOG2E = 1.4426950408889634
NZ = 8
NY = 4
F32 = jnp.float32
BF16 = jnp.bfloat16
MESH = pl.DeviceIdType.MESH
VMEM = pl.BlockSpec(memory_space=pltpu.VMEM)
ANY = pl.BlockSpec(memory_space=pl.ANY)
SMEM = pl.BlockSpec(memory_space=pltpu.SMEM)


def remote(src, dst, send, recv, device):
    return pltpu.make_async_remote_copy(
        src_ref=src, dst_ref=dst, send_sem=send, recv_sem=recv, device_id=device, device_id_type=MESH
    )


def meet(peers):
    barrier = pltpu.get_barrier_semaphore()
    for peer in peers:
        pl.semaphore_signal(barrier, inc=1, device_id=peer, device_id_type=MESH)
    pl.semaphore_wait(barrier, len(peers))


def layer_kernel(
    q_ref,
    k_ref,
    v_ref,
    gate_ref,
    up_ref,
    lam_ref,
    gain_ref,
    resid_ref,
    ow_ref,
    ng_ref,
    cw_ref,
    cb_ref,
    dw_ref,
    out_ref,
    *,
    gug,
    kbuf,
    vbuf,
    qbuf,
    kk,
    vv,
    qbd,
    top,
    total,
    acc,
    lse,
    part,
    relay,
    landed,
    hall,
    nall,
    am,
    ssq,
    big,
    gpad,
    gedge,
    halo,
    hid,
    dall,
    psib,
    rsib,
    pout,
    relayed,
    rout,
    keep,
    ks,
    kr,
    vs,
    vr,
    qs,
    qr,
    gs,
    gr,
    ya_s,
    ya_r,
    yb_s,
    yb_r,
    hs,
    hr,
    hz_s,
    hz_r,
    ls,
    lr,
    ms,
    mr,
    xs,
    xr,
    cs,
    cr,
    ts,
    tr,
    es,
    er,
    ys,
    yrr,
    zs,
    zrr,
    as_,
    ar,
    dya_s,
    dya_r,
    dyb_s,
    dyb_r,
    bs,
    br,
    ps,
    pr,
):
    sp, tp = lax.axis_index("sp"), lax.axis_index("tp")
    z, y = sp // NY, sp % NY
    length = q_ref.shape[0]
    cols = 2 * length
    half = length // 2
    units = gate_ref.shape[1]
    whole = units // 128 * 128
    rest = units - whole
    first = pl.ds(0, 48)
    last = pl.ds(48, 16)

    def index(dz, dy):
        return ((z + dz) % NZ) * NY + (y + dy) % NY

    def device(dz, dy):
        return (index(dz, dy), tp)

    zr, zl = device(1, 0), device(7, 0)
    yr, yl = device(0, 1), device(0, 3)
    gug[sp, :, 0:whole] = gate_ref[:, 0:whole]
    gug[sp, :, whole : 2 * whole] = up_ref[:, 0:whole]
    gug[sp, :, 2 * whole :] = jnp.concatenate([gate_ref[:, whole:], up_ref[:, whole:]], axis=1)
    dall[sp] = dw_ref[...]
    am[...] = resid_ref[...].astype(F32)
    x, c = tp // 2, tp % 2
    width = resid_ref.shape[1]
    units_rows = dw_ref.shape[0]

    def xdev(dx, other=0):
        return (sp, ((x + dx) % 4) * 2 + (c + other) % 2)

    xr_, xl_, sib = xdev(1), xdev(3), xdev(0, 1)
    after, before_ = ((sp + 1) % (NZ * NY), tp), ((sp + NZ * NY - 1) % (NZ * NY), tp)
    tp_peers = [(sp, (tp + i) % 8) for i in range(1, 8)]
    meet([zr, zl, yr, yl, device(0, 2)] + tp_peers + [after, before_])
    started = []

    def go(copy):
        copy.start()
        started.append(copy)
        return copy

    def arrive(copies):
        for copy in copies:
            copy.wait_recv()

    def kslot(s):
        return k_ref if s == 0 else kbuf.at[s]

    def vslot(s):
        return v_ref if s == 0 else vbuf.at[s]

    def send_kv(t):
        right, left = t, (8 - t) % 8
        out = [go(remote(kslot(right), kbuf.at[t + 1], ks.at[0, t], kr.at[t + 1], zr))]
        if t < 3:
            out.append(go(remote(kslot(left), kbuf.at[7 - t], ks.at[1, t], kr.at[7 - t], zl)))
            out.append(go(remote(vslot(right), vbuf.at[t + 1], vs.at[0, t], vr.at[t + 1], zr)))
        out.append(go(remote(vslot(left), vbuf.at[7 - t], vs.at[1, t], vr.at[7 - t], zl)))
        return out

    def source(s, rows):
        return gug.at[index(8 - s, 0), rows]

    def parts(s):
        return (pl.ds(0, 16), pl.ds(16, 32)) if s % 2 == 0 else (pl.ds(0, 32), pl.ds(32, 16))

    def send_g(t):
        right, left = t, (8 - t) % 8
        rows_r, rows_l = parts(0) if t == 3 else (first, first)
        return [
            go(remote(source(right, rows_r), gug.at[index(8 - right, 0), rows_r], gs.at[0, t], gr.at[0, t], zr)),
            go(remote(source(left, rows_l), gug.at[index(8 - left, 0), rows_l], gs.at[1, t], gr.at[1, t], zl)),
        ]

    def send_ya(s):
        dst = gug.at[index(8 - s, 0), first]
        return [
            go(remote(source(s, first), dst, ya_s.at[0, s], ya_r.at[0, s], yr)),
            go(remote(source(s, first), dst, ya_s.at[1, s], ya_r.at[1, s], yl)),
        ]

    def send_yb(s):
        rows_r, rows_l = parts(s)
        a = gug.at[index(8 - s, 3), rows_r]
        b = gug.at[index(8 - s, 1), rows_l]
        return [
            go(remote(a, a, yb_s.at[0, s], yb_r.at[0, s], yr)),
            go(remote(b, b, yb_s.at[1, s], yb_r.at[1, s], yl)),
        ]

    def send_h(t):
        right, left = ((z + 8 - t) % NZ) * NY, ((z + t) % NZ) * NY
        if t < 3:
            a, b = gug.at[pl.ds(right, NY), last], gug.at[pl.ds(left, NY), last]
        else:
            a, b = gug.at[pl.ds(right, 2), last], gug.at[pl.ds(left + 2, 2), last]
        return [
            go(remote(a, a, hz_s.at[0, t], hz_r.at[0, t], zr)),
            go(remote(b, b, hz_s.at[1, t], hz_r.at[1, t], zl)),
        ]

    da, dya, dyb, dz = [], {}, {}, []
    turn = units_rows // 2
    early, late = pl.ds(0, turn), pl.ds(turn, turn)
    upper_q, lower_q = pl.ds(0, turn // 2), pl.ds(turn // 2, turn // 2)

    def dsource(s, rows):
        return dall.at[index(8 - s, 0), rows]

    def send_a(t):
        right, left = t, (8 - t) % 8
        rows_r, rows_l = (upper_q, lower_q) if t == 3 else (early, early)
        return [
            go(remote(dsource(right, rows_r), dall.at[index(8 - right, 0), rows_r], as_.at[0, t], ar.at[0, t], zr)),
            go(remote(dsource(left, rows_l), dall.at[index(8 - left, 0), rows_l], as_.at[1, t], ar.at[1, t], zl)),
        ]

    def send_dya(s):
        dst = dall.at[index(8 - s, 0), early]
        return [
            go(remote(dsource(s, early), dst, dya_s.at[0, s], dya_r.at[0, s], yr)),
            go(remote(dsource(s, early), dst, dya_s.at[1, s], dya_r.at[1, s], yl)),
        ]

    def send_dyb(s):
        a = dall.at[index(8 - s, 3), upper_q]
        b = dall.at[index(8 - s, 1), lower_q]
        return [
            go(remote(a, a, dyb_s.at[0, s], dyb_r.at[0, s], yr)),
            go(remote(b, b, dyb_s.at[1, s], dyb_r.at[1, s], yl)),
        ]

    def send_d(t):
        right, left = ((z + 8 - t) % NZ) * NY, ((z + t) % NZ) * NY
        if t < 3:
            a, b = dall.at[pl.ds(right, NY), late], dall.at[pl.ds(left, NY), late]
        else:
            a, b = dall.at[pl.ds(right, 2), late], dall.at[pl.ds(left + 2, 2), late]
        return [
            go(remote(a, a, zs.at[0, t], zrr.at[0, t], zr)),
            go(remote(b, b, zs.at[1, t], zrr.at[1, t], zl)),
        ]

    def gather(stack, k):
        mine = stack.at[tp]
        one = [
            go(remote(mine, mine, xs.at[k, 0], xr.at[k, 0], xr_)),
            go(remote(mine, mine, xs.at[k, 1], xr.at[k, 1], xl_)),
        ]
        core = [go(remote(mine, mine, cs.at[k, 0], cr.at[k, 0], sib))]
        yield None
        arrive(core)
        yield 0
        from_left = stack.at[((x + 3) % 4) * 2 + c]
        from_right = stack.at[((x + 1) % 4) * 2 + c]
        upper, lower = pl.ds(0, half), pl.ds(half, half)
        arrive(one[:1])
        two = [go(remote(from_left.at[upper], from_left.at[upper], xs.at[k, 2], xr.at[k, 2], xr_))]
        core.append(go(remote(from_left, from_left, cs.at[k, 1], cr.at[k, 1], sib)))
        arrive(one[1:])
        two.append(go(remote(from_right.at[lower], from_right.at[lower], xs.at[k, 3], xr.at[k, 3], xl_)))
        core.append(go(remote(from_right, from_right, cs.at[k, 2], cr.at[k, 2], sib)))
        arrive(core[1:2])
        yield 3
        arrive(core[2:3])
        yield 1
        far = stack.at[((x + 2) % 4) * 2 + c]
        arrive(two[:1])
        core.append(go(remote(far.at[upper], far.at[upper], cs.at[k, 3], cr.at[k, 3], sib)))
        arrive(two[1:])
        core.append(go(remote(far.at[lower], far.at[lower], cs.at[k, 4], cr.at[k, 4], sib)))
        arrive(core[3:5])
        yield 2

    def relay_a(t):
        arrive(da[t])
        if t < 3:
            da.append(send_a(t + 1))
        for s in (t + 1, 7 - t) if t < 3 else (4,):
            dya[s] = send_dya(s)

    def relay_y(*slots):
        for s in slots:
            arrive(dya[s])
            dyb[s] = send_dyb(s)

    def relay_d(t, along=None):
        arrive(along if t == 0 else dz[t - 1])
        dz.append(send_d(t))

    qa = [
        go(remote(q_ref, qbuf.at[1], qs.at[0], qr.at[0], yr)),
        go(remote(q_ref, qbuf.at[3], qs.at[1], qr.at[1], yl)),
    ]
    kv = [send_kv(0)]
    g = [send_g(0)]
    hy = [
        go(remote(gug.at[sp, last], gug.at[sp, last], hs.at[i - 1], hr.at[i - 1], device(0, i)))
        for i in (1, 3, 2)
    ]
    ya = {0: send_ya(0)}
    yb = {}
    h = []

    top[...] = jnp.full(top.shape, -1e30, F32)
    total[...] = jnp.zeros(total.shape, F32)
    acc[...] = jnp.zeros(acc.shape, F32)
    row = lax.broadcasted_iota(jnp.int32, (2 * HD, 128), 0)

    def lay_queries(src, slot):
        for j in range(length // 128):
            turned = src[j * 128 : (j + 1) * 128, :].astype(F32).T * (LOG2E * HD**-0.5)
            for m in range(2):
                at = slot * cols + j * 256 + m * 128
                kept = jnp.where((row < HD) if m == 0 else (row >= HD), turned, 0.0)
                high = kept.astype(BF16)
                qbd[0:128, at : at + 128] = high
                qbd[128:256, at : at + 128] = (kept - high.astype(F32)).astype(BF16)

    def stage(slots):
        for n, s in enumerate(slots):
            kb = kslot(s)[...]
            kk[n * length : (n + 1) * length, 0:128] = kb
            kk[n * length : (n + 1) * length, 128:256] = kb
            vv[n * length : (n + 1) * length, :] = vslot(s)[...]

    def attend(count, begin, end):
        keys = count * length

        def tile(i, carry):
            at = pl.ds(pl.multiple_of(i * cols, cols), cols)
            scores = jnp.dot(kk[0:keys, :], qbd[:, at], preferred_element_type=F32)
            before = top[0:1, at]
            now = jnp.maximum(before, jnp.max(scores, axis=0, keepdims=True))
            shifted = jnp.exp2(scores - now)
            factor = jnp.exp2(before - now)
            top[0:1, at] = now
            total[0:1, at] = total[0:1, at] * factor + jnp.sum(shifted, axis=0, keepdims=True)
            acc[:, at] = acc[:, at] * factor + lax.dot_general(
                vv[0:keys, :],
                shifted.astype(BF16),
                (((0,), (0,)), ((), ())),
                preferred_element_type=F32,
            )
            return carry

        lax.fori_loop(begin, end, tile, 0)

    lay_queries(q_ref, 0)
    stage([0])
    attend(1, 0, 1)
    arrive(qa)
    low, high_rows = pl.ds(0, half), pl.ds(half, half)
    qb = [
        go(remote(qbuf.at[1, low], qbuf.at[2, low], qs.at[2], qr.at[2], yr)),
        go(remote(qbuf.at[3, high_rows], qbuf.at[2, high_rows], qs.at[3], qr.at[3], yl)),
    ]
    lay_queries(qbuf.at[1], 1)
    lay_queries(qbuf.at[3], 3)
    attend(1, 1, 2)
    attend(1, 3, 4)
    arrive(qb)
    lay_queries(qbuf.at[2], 2)
    attend(1, 2, 3)

    for t in range(1, 5):
        arrive(kv[t - 1])
        if t < 4:
            kv.append(send_kv(t))
        slots = [t, 8 - t] if t < 4 else [4]
        stage(slots)
        attend(len(slots), 0, 2)
        arrive(g[t - 1])
        if t < 4:
            g.append(send_g(t))
            for s in slots:
                ya[s] = send_ya(s)
            for s in (0,) if t == 1 else (t - 1, 9 - t):
                arrive(ya[s])
                yb[s] = send_yb(s)
        else:
            arrive(hy)
            h.append(send_h(0))
        attend(len(slots), 2, 4)

    for slot in range(4):
        for n in range(2):
            at = slice(slot * cols + n * length, slot * cols + (n + 1) * length)
            lse[0, 2 * slot + n : 2 * slot + n + 1, :] = top[0:1, at] + jnp.log2(total[0:1, at])
    stats = [
        go(remote(lse.at[0], lse.at[4 - i], ls.at[i - 1], lr.at[3 - i], device(0, i))) for i in (2, 1, 3)
    ]
    arrive(stats)
    weights = {}
    for slot in range(4):
        for n in range(2):
            logs = []
            for e in range(4):
                r = 2 * ((slot + e) % 4) + n
                logs.append(lse[e, r : r + 1, :])
            highest = jnp.maximum(jnp.maximum(logs[0], logs[1]), jnp.maximum(logs[2], logs[3]))
            shares = [jnp.exp2(v - highest) for v in logs]
            at = slice(slot * cols + n * length, slot * cols + (n + 1) * length)
            weights[slot, n] = shares[0] / ((shares[0] + shares[1] + shares[2] + shares[3]) * total[0:1, at])

    def mixture(slot, rows):
        out = []
        for j in range(length // 128):
            maps = []
            for m in range(2):
                at = j * 256 + m * 128
                w = weights[slot, at // length][:, at % length : at % length + 128]
                maps.append(acc[rows, slot * cols + at : slot * cols + at + 128] * w)
            out.append(maps[0] - lam_ref[0] * maps[1])
        return jnp.concatenate(out, axis=1)

    up_rows, low_rows = slice(0, 64), slice(64, 128)
    at_up, at_low = pl.ds(0, 64), pl.ds(64, 64)
    part[2, up_rows, :] = mixture(2, up_rows).astype(BF16)
    part[2, low_rows, :] = mixture(2, low_rows).astype(BF16)
    over = [
        go(remote(part.at[2, at_up], relay.at[0], ms.at[0], mr.at[0], yr)),
        go(remote(part.at[2, at_low], relay.at[1], ms.at[1], mr.at[1], yl)),
    ]
    part[3, low_rows, :] = mixture(3, low_rows).astype(BF16)
    part[1, up_rows, :] = mixture(1, up_rows).astype(BF16)
    ends = [
        go(remote(part.at[3, at_low], landed.at[0, at_low], ms.at[2], mr.at[2], yr)),
        go(remote(part.at[1, at_up], landed.at[1, at_up], ms.at[3], mr.at[3], yl)),
    ]
    third, firsts = mixture(3, up_rows), mixture(1, low_rows)
    arrive(h[0])
    h.append(send_h(1))
    arrive(over)
    part[3, up_rows, :] = (third + relay[0].astype(F32)).astype(BF16)
    part[1, low_rows, :] = (firsts + relay[1].astype(F32)).astype(BF16)
    ends += [
        go(remote(part.at[3, at_up], landed.at[0, at_up], ms.at[4], mr.at[4], yr)),
        go(remote(part.at[1, at_low], landed.at[1, at_low], ms.at[5], mr.at[5], yl)),
    ]
    ya[4] = send_ya(4)
    for s in (3, 5):
        arrive(ya[s])
        yb[s] = send_yb(s)
    da.append(send_a(0))
    dya[0] = send_dya(0)
    mixed = mixture(0, slice(0, 128))
    arrive(ends)
    mixed = mixed + (landed[0].astype(F32) + landed[1].astype(F32))
    spread = jnp.mean(mixed * mixed, axis=0, keepdims=True)
    normed = mixed * lax.rsqrt(spread + 1e-06)
    gain = gain_ref[...][None, :] * 0.8
    for j in range(length // 128):
        at = slice(j * 128, (j + 1) * 128)
        hall[tp, at, :] = (normed[:, at].T * gain).astype(BF16)
    heads = gather(hall, 0)
    next(heads)
    along = [
        go(remote(dall.at[sp, late], dall.at[sp, late], ys.at[i - 1], yrr.at[i - 1], device(0, i)))
        for i in (1, 3, 2)
    ]
    arrive(h[1])
    h.append(send_h(2))
    arrive(ya[4])
    yb[4] = send_yb(4)
    for n, dx in enumerate(heads):
        chip = (x + dx) % 4
        for core in range(2):
            rows = pl.ds(pl.multiple_of((chip * 2 + core) * VD, VD), VD)
            am[...] += jnp.dot(hall[chip * 2 + core], ow_ref[rows, :], preferred_element_type=F32)
        if n == 0:
            relay_a(0)
            relay_d(0, along)
        elif n == 2:
            arrive(h[2])
            h.append(send_h(3))
            relay_a(1)
            relay_y(0)
    value = am[...]
    nall[tp] = (value * ng_ref[...][None, :]).astype(BF16)
    rows_in = gather(nall, 1)
    next(rows_in)
    square = value * value
    square = square[:, 0:128] + square[:, 128:256]
    for j in range(length // 128):
        ssq[tp, j : j + 1, :] = jnp.sum(square[j * 128 : (j + 1) * 128, :].T, axis=0, keepdims=True)
    ssq[tp, length // 128 :, :] = jnp.zeros((8 - length // 128, 128), F32)
    tiny = [
        go(remote(ssq.at[tp], ssq.at[tp], ts.at[i - 1], tr.at[i - 1], (sp, (tp + i) % 8)))
        for i in range(1, 8)
    ]
    relay_a(2)
    relay_y(1, 7)
    relay_d(1)
    for s in range(8):
        arrive(yb[s])
    arrive(h[3])

    def product(chip):
        a = jnp.concatenate([nall[chip * 2], nall[chip * 2 + 1]], axis=1)
        per_chip = 2 * width // units_rows
        return jnp.dot(a, gug[pl.ds(chip * per_chip, per_chip)].reshape(2 * width, 2 * units), preferred_element_type=F32)

    for n, dx in enumerate(rows_in):
        if n == 0:
            big[...] = product((x + dx) % 4)
            relay_a(3)
            relay_y(2, 6)
        else:
            big[...] += product((x + dx) % 4)
        if n == 2:
            relay_d(2)
            relay_y(3, 5)
    relay_d(3)
    relay_y(4)
    arrive(tiny)
    squares = ssq[0]
    for i in range(1, 8):
        squares = squares + ssq[i]
    factor = lax.rsqrt(squares * (1.0 / D) + 1e-06)
    for j in range(length // 128):
        rows = slice(j * 128, (j + 1) * 128)
        column = jnp.broadcast_to(factor[j : j + 1, :], (128, 128)).T[:, 0:1]
        scaled = big[rows, :] * column
        gate = jnp.concatenate([scaled[:, 0:whole], scaled[:, 2 * whole : 2 * whole + rest]], axis=1)
        gpad[8 + j * 128 : 8 + (j + 1) * 128, :] = gate.astype(BF16).astype(F32)
        big[rows, whole:] = scaled[:, whole:]
    gedge[0] = gpad[8:24, :].astype(BF16)
    gedge[1] = gpad[8 + length - 16 : 8 + length, :].astype(BF16)
    edge = [
        go(remote(gedge.at[1], halo.at[0], es.at[0], er.at[0], after)),
        go(remote(gedge.at[0], halo.at[1], es.at[1], er.at[1], before_)),
    ]

    def convolve(j):
        rows = slice(j * 128, (j + 1) * 128)
        at = 8 + j * 128
        conv = (
            gpad[at - 1 : at + 127, :] * cw_ref[0:1, :]
            + gpad[at : at + 128, :] * cw_ref[1:2, :]
            + gpad[at + 1 : at + 129, :] * cw_ref[2:3, :]
            + cb_ref[...][None, :]
        )
        up = jnp.concatenate([big[rows, whole : 2 * whole], big[rows, 2 * whole + rest :]], axis=1)
        hid[rows, :] = (conv / (1.0 + jnp.exp(-conv)) * up).astype(BF16)

    for j in range(1, length // 128 - 1):
        convolve(j)
    arrive(edge)
    gpad[7:8, :] = jnp.where(sp == 0, 0.0, halo[0].astype(F32)[15:16, :])
    gpad[8 + length : 9 + length, :] = jnp.where(sp == NZ * NY - 1, 0.0, halo[1].astype(F32)[0:1, :])
    convolve(0)
    convolve(length // 128 - 1)

    for s in range(8):
        arrive(dyb[s])
    arrive(dz[3])
    per = width // units_rows

    def down(target):
        w = dall[pl.ds(target * per, per)].reshape(width, units)
        return lax.dot_general(
            hid[...], w, (((1,), (1,)), ((), ())), preferred_element_type=F32
        )

    order = (2, 1, 3, 0)
    crossing = {}
    for dx in order:
        psib[dx] = down(((x + dx) % 4) * 2 + (1 - c)).astype(BF16)
        crossing[dx] = go(remote(psib.at[dx], rsib.at[dx], bs.at[dx], br.at[dx], sib))
    upper, lower = slice(0, half), slice(half, length)
    at_upper, at_lower = pl.ds(0, half), pl.ds(half, half)
    ends = []
    for dx in order:
        piece = down(((x + dx) % 4) * 2 + c)
        arrive([crossing[dx]])
        piece = piece + rsib[dx].astype(F32)
        if dx == 2:
            pout[2] = piece.astype(BF16)
            over = [
                go(remote(pout.at[2, at_upper], relayed.at[0], ps.at[0], pr.at[0], xr_)),
                go(remote(pout.at[2, at_lower], relayed.at[1], ps.at[1], pr.at[1], xl_)),
            ]
        elif dx == 1:
            pout[1, lower, :] = piece[lower, :].astype(BF16)
            ends.append(go(remote(pout.at[1, at_lower], rout.at[0, at_lower], ps.at[2], pr.at[2], xr_)))
            keep[0] = piece[upper, :]
        elif dx == 3:
            pout[3, upper, :] = piece[upper, :].astype(BF16)
            ends.append(go(remote(pout.at[3, at_upper], rout.at[1, at_upper], ps.at[3], pr.at[3], xl_)))
            keep[1] = piece[lower, :]
            arrive(over)
            pout[1, upper, :] = (keep[0] + relayed[0].astype(F32)).astype(BF16)
            ends.append(go(remote(pout.at[1, at_upper], rout.at[0, at_upper], ps.at[4], pr.at[4], xr_)))
            pout[3, lower, :] = (keep[1] + relayed[1].astype(F32)).astype(BF16)
            ends.append(go(remote(pout.at[3, at_lower], rout.at[1, at_lower], ps.at[5], pr.at[5], xl_)))
        else:
            am[...] += piece
    arrive(ends)
    out_ref[...] = (am[...] + (rout[0].astype(F32) + rout[1].astype(F32))).astype(BF16)
    for copy in started:
        copy.wait_send()


def layer(q, k, v, gate, up, lam, gain, resid, ow, ng, cw, cb, dw):
    length, width = resid.shape
    cols = 2 * length
    rows, units = gate.shape
    half = length // 2
    dma, vmem = pltpu.SemaphoreType.DMA, pltpu.VMEM
    scratch = dict(
        gug=vmem((NZ * NY, rows, 2 * units), BF16),
        kbuf=vmem((8, length, 128), BF16),
        vbuf=vmem((8, length, 128), BF16),
        qbuf=vmem((4, length, 128), BF16),
        kk=vmem((2 * length, 256), BF16),
        vv=vmem((2 * length, 128), BF16),
        qbd=vmem((256, 4 * cols), BF16),
        top=vmem((8, 4 * cols), F32),
        total=vmem((8, 4 * cols), F32),
        acc=vmem((VD, 4 * cols), F32),
        lse=vmem((4, 8, length), F32),
        part=vmem((4, VD, length), BF16),
        relay=vmem((2, VD // 2, length), BF16),
        landed=vmem((2, VD, length), BF16),
        hall=vmem((8, length, VD), BF16),
        nall=vmem((8, length, width), BF16),
        am=vmem((length, width), F32),
        ssq=vmem((8, 8, 128), F32),
        big=vmem((length, 2 * units), F32),
        gpad=vmem((length + 16, units), F32),
        gedge=vmem((2, 16, units), BF16),
        halo=vmem((2, 16, units), BF16),
        hid=vmem((length, units), BF16),
        dall=vmem((NZ * NY, *dw.shape), BF16),
        psib=vmem((4, length, width), BF16),
        rsib=vmem((4, length, width), BF16),
        pout=vmem((4, length, width), BF16),
        relayed=vmem((2, half, width), BF16),
        rout=vmem((2, length, width), BF16),
        keep=vmem((2, half, width), F32),
    )
    semaphores = dict(
        ks=(2, 4), kr=(8,), vs=(2, 4), vr=(8,), qs=(4,), qr=(4,), gs=(2, 4), gr=(2, 4),
        ya_s=(2, 8), ya_r=(2, 8), yb_s=(2, 8), yb_r=(2, 8), hs=(3,), hr=(3,), hz_s=(2, 4), hz_r=(2, 4),
        ls=(3,), lr=(3,), ms=(6,), mr=(6,), xs=(2, 4), xr=(2, 4), cs=(2, 5), cr=(2, 5), ts=(7,), tr=(7,),
        es=(2,), er=(2,), ys=(3,), yrr=(3,), zs=(2, 4), zrr=(2, 4), as_=(2, 4), ar=(2, 4),
        dya_s=(2, 8), dya_r=(2, 8), dyb_s=(2, 8), dyb_r=(2, 8), bs=(4,), br=(4,), ps=(6,), pr=(6,),
    )
    return pl.pallas_call(
        layer_kernel,
        name="layer",
        out_shape=jax.ShapeDtypeStruct((length, width), BF16),
        in_specs=[VMEM] * 5 + [SMEM] + [VMEM] * 7,
        out_specs=VMEM,
        scratch_shapes=dict(scratch, **{n: dma(shape) for n, shape in semaphores.items()}),
        compiler_params=pltpu.CompilerParams(
            collective_id=0, has_side_effects=True, vmem_limit_bytes=63 * 2**20
        ),
    )(q, k, v, gate, up, lam, gain, resid, ow, ng, cw, cb, dw)


def on_device(
    resid,
    queries,
    keys,
    values,
    mix_lambda,
    head_gain,
    out_weight,
    norm_gain,
    gate_weight,
    up_weight,
    conv_weight,
    conv_bias,
    down_weight,
):
    return layer(
        queries,
        keys,
        values,
        gate_weight,
        up_weight,
        mix_lambda,
        head_gain,
        resid,
        out_weight,
        norm_gain,
        conv_weight,
        conv_bias,
        down_weight.T,
    )


def solution(mesh):
    return jax.shard_map(
        on_device,
        mesh=mesh,
        in_specs=(
            P("sp", "tp"),
            P("sp", "tp"),
            P("sp", "tp"),
            P("sp", "tp"),
            P("tp"),
            P(),
            P(None, "tp"),
            P("tp"),
            P("sp", "tp"),
            P("sp", "tp"),
            P(None, "tp"),
            P("tp"),
            P("tp", "sp"),
        ),
        out_specs=P("sp", "tp"),
        check_vma=False,
    )
```

```python
import jax
import jax.numpy as jnp
from jax import lax
from jax.experimental import pallas as pl
from jax.experimental.pallas import tpu as pltpu
from jax.sharding import PartitionSpec as P

D = 2048
HD = 64
VD = 128
LOG2E = 1.4426950408889634
NZ = 8
NY = 4
F32 = jnp.float32
BF16 = jnp.bfloat16
MESH = pl.DeviceIdType.MESH
VMEM = pl.BlockSpec(memory_space=pltpu.VMEM)
ANY = pl.BlockSpec(memory_space=pl.ANY)
SMEM = pl.BlockSpec(memory_space=pltpu.SMEM)


def remote(src, dst, send, recv, device):
    return pltpu.make_async_remote_copy(
        src_ref=src, dst_ref=dst, send_sem=send, recv_sem=recv, device_id=device, device_id_type=MESH
    )


def meet(peers):
    barrier = pltpu.get_barrier_semaphore()
    for peer in peers:
        pl.semaphore_signal(barrier, inc=1, device_id=peer, device_id_type=MESH)
    pl.semaphore_wait(barrier, len(peers))


def layer_kernel(
    q_ref,
    k_ref,
    v_ref,
    gate_ref,
    up_ref,
    lam_ref,
    gain_ref,
    resid_ref,
    ow_ref,
    ng_ref,
    cw_ref,
    cb_ref,
    dw_ref,
    out_ref,
    *,
    gug,
    kbuf,
    vbuf,
    qbuf,
    kk,
    vv,
    qbd,
    top,
    total,
    acc,
    lse,
    part,
    relay,
    landed,
    hall,
    nall,
    am,
    ssq,
    big,
    gpad,
    gedge,
    halo,
    hid,
    dall,
    psib,
    rsib,
    pout,
    relayed,
    rout,
    keep,
    ks,
    kr,
    vs,
    vr,
    qs,
    qr,
    gs,
    gr,
    ya_s,
    ya_r,
    yb_s,
    yb_r,
    hs,
    hr,
    hz_s,
    hz_r,
    ls,
    lr,
    ms,
    mr,
    xs,
    xr,
    cs,
    cr,
    ts,
    tr,
    es,
    er,
    ys,
    yrr,
    zs,
    zrr,
    as_,
    ar,
    dya_s,
    dya_r,
    dyb_s,
    dyb_r,
    bs,
    br,
    ps,
    pr,
):
    sp, tp = lax.axis_index("sp"), lax.axis_index("tp")
    z, y = sp // NY, sp % NY
    length = q_ref.shape[0]
    cols = 2 * length
    half = length // 2
    units = gate_ref.shape[1]
    whole = units // 128 * 128
    rest = units - whole
    first = pl.ds(0, 48)
    last = pl.ds(48, 16)

    def index(dz, dy):
        return ((z + dz) % NZ) * NY + (y + dy) % NY

    def device(dz, dy):
        return (index(dz, dy), tp)

    zr, zl = device(1, 0), device(7, 0)
    yr, yl = device(0, 1), device(0, 3)
    gug[sp, :, 0:whole] = gate_ref[:, 0:whole]
    gug[sp, :, whole : 2 * whole] = up_ref[:, 0:whole]
    gug[sp, :, 2 * whole :] = jnp.concatenate([gate_ref[:, whole:], up_ref[:, whole:]], axis=1)
    dall[sp] = dw_ref[...]
    am[...] = resid_ref[...].astype(F32)
    x, c = tp // 2, tp % 2
    width = resid_ref.shape[1]
    units_rows = dw_ref.shape[0]

    def xdev(dx, other=0):
        return (sp, ((x + dx) % 4) * 2 + (c + other) % 2)

    xr_, xl_, sib = xdev(1), xdev(3), xdev(0, 1)
    after, before_ = ((sp + 1) % (NZ * NY), tp), ((sp + NZ * NY - 1) % (NZ * NY), tp)
    tp_peers = [(sp, (tp + i) % 8) for i in range(1, 8)]
    meet([zr, zl, yr, yl, device(0, 2)] + tp_peers + [after, before_])
    started = []

    def go(copy):
        copy.start()
        started.append(copy)
        return copy

    def arrive(copies):
        for copy in copies:
            copy.wait_recv()

    def kslot(s):
        return k_ref if s == 0 else kbuf.at[s]

    def vslot(s):
        return v_ref if s == 0 else vbuf.at[s]

    def send_kv(t):
        right, left = t, (8 - t) % 8
        out = [go(remote(kslot(right), kbuf.at[t + 1], ks.at[0, t], kr.at[t + 1], zr))]
        if t < 3:
            out.append(go(remote(kslot(left), kbuf.at[7 - t], ks.at[1, t], kr.at[7 - t], zl)))
            out.append(go(remote(vslot(right), vbuf.at[t + 1], vs.at[0, t], vr.at[t + 1], zr)))
        out.append(go(remote(vslot(left), vbuf.at[7 - t], vs.at[1, t], vr.at[7 - t], zl)))
        return out

    def source(s, rows):
        return gug.at[index(8 - s, 0), rows]

    def parts(s):
        return (pl.ds(0, 16), pl.ds(16, 32)) if s % 2 == 0 else (pl.ds(0, 32), pl.ds(32, 16))

    def send_g(t):
        right, left = t, (8 - t) % 8
        rows_r, rows_l = parts(0) if t == 3 else (first, first)
        return [
            go(remote(source(right, rows_r), gug.at[index(8 - right, 0), rows_r], gs.at[0, t], gr.at[0, t], zr)),
            go(remote(source(left, rows_l), gug.at[index(8 - left, 0), rows_l], gs.at[1, t], gr.at[1, t], zl)),
        ]

    def send_ya(s):
        dst = gug.at[index(8 - s, 0), first]
        return [
            go(remote(source(s, first), dst, ya_s.at[0, s], ya_r.at[0, s], yr)),
            go(remote(source(s, first), dst, ya_s.at[1, s], ya_r.at[1, s], yl)),
        ]

    def send_yb(s):
        rows_r, rows_l = parts(s)
        a = gug.at[index(8 - s, 3), rows_r]
        b = gug.at[index(8 - s, 1), rows_l]
        return [
            go(remote(a, a, yb_s.at[0, s], yb_r.at[0, s], yr)),
            go(remote(b, b, yb_s.at[1, s], yb_r.at[1, s], yl)),
        ]

    def send_h(t):
        right, left = ((z + 8 - t) % NZ) * NY, ((z + t) % NZ) * NY
        if t < 3:
            a, b = gug.at[pl.ds(right, NY), last], gug.at[pl.ds(left, NY), last]
        else:
            a, b = gug.at[pl.ds(right, 2), last], gug.at[pl.ds(left + 2, 2), last]
        return [
            go(remote(a, a, hz_s.at[0, t], hz_r.at[0, t], zr)),
            go(remote(b, b, hz_s.at[1, t], hz_r.at[1, t], zl)),
        ]

    da, dya, dyb, dz = [], {}, {}, []
    turn = units_rows // 2
    early, late = pl.ds(0, turn), pl.ds(turn, turn)
    upper_q, lower_q = pl.ds(0, turn // 2), pl.ds(turn // 2, turn // 2)

    def dsource(s, rows):
        return dall.at[index(8 - s, 0), rows]

    def send_a(t):
        right, left = t, (8 - t) % 8
        rows_r, rows_l = (upper_q, lower_q) if t == 3 else (early, early)
        return [
            go(remote(dsource(right, rows_r), dall.at[index(8 - right, 0), rows_r], as_.at[0, t], ar.at[0, t], zr)),
            go(remote(dsource(left, rows_l), dall.at[index(8 - left, 0), rows_l], as_.at[1, t], ar.at[1, t], zl)),
        ]

    def send_dya(s):
        dst = dall.at[index(8 - s, 0), early]
        return [
            go(remote(dsource(s, early), dst, dya_s.at[0, s], dya_r.at[0, s], yr)),
            go(remote(dsource(s, early), dst, dya_s.at[1, s], dya_r.at[1, s], yl)),
        ]

    def send_dyb(s):
        a = dall.at[index(8 - s, 3), upper_q]
        b = dall.at[index(8 - s, 1), lower_q]
        return [
            go(remote(a, a, dyb_s.at[0, s], dyb_r.at[0, s], yr)),
            go(remote(b, b, dyb_s.at[1, s], dyb_r.at[1, s], yl)),
        ]

    def send_d(t):
        right, left = ((z + 8 - t) % NZ) * NY, ((z + t) % NZ) * NY
        if t < 3:
            a, b = dall.at[pl.ds(right, NY), late], dall.at[pl.ds(left, NY), late]
        else:
            a, b = dall.at[pl.ds(right, 2), late], dall.at[pl.ds(left + 2, 2), late]
        return [
            go(remote(a, a, zs.at[0, t], zrr.at[0, t], zr)),
            go(remote(b, b, zs.at[1, t], zrr.at[1, t], zl)),
        ]

    quarter = half // 2

    def gather(stack, k, begin):
        here = pl.ds(begin, half)
        upper, lower = pl.ds(begin, quarter), pl.ds(begin + quarter, quarter)
        mine = stack.at[tp, here]
        one = [
            go(remote(mine, mine, xs.at[k, 0], xr.at[k, 0], xr_)),
            go(remote(mine, mine, xs.at[k, 1], xr.at[k, 1], xl_)),
        ]
        core = [go(remote(mine, mine, cs.at[k, 0], cr.at[k, 0], sib))]
        yield None
        arrive(core)
        yield 0
        left, right = ((x + 3) % 4) * 2 + c, ((x + 1) % 4) * 2 + c
        arrive(one[:1])
        two = [go(remote(stack.at[left, upper], stack.at[left, upper], xs.at[k, 2], xr.at[k, 2], xr_))]
        core.append(go(remote(stack.at[left, here], stack.at[left, here], cs.at[k, 1], cr.at[k, 1], sib)))
        arrive(one[1:])
        two.append(go(remote(stack.at[right, lower], stack.at[right, lower], xs.at[k, 3], xr.at[k, 3], xl_)))
        core.append(go(remote(stack.at[right, here], stack.at[right, here], cs.at[k, 2], cr.at[k, 2], sib)))
        yield None
        arrive(core[1:2])
        yield 3
        arrive(core[2:3])
        yield 1
        far = ((x + 2) % 4) * 2 + c
        arrive(two[:1])
        core.append(go(remote(stack.at[far, upper], stack.at[far, upper], cs.at[k, 3], cr.at[k, 3], sib)))
        arrive(two[1:])
        core.append(go(remote(stack.at[far, lower], stack.at[far, lower], cs.at[k, 4], cr.at[k, 4], sib)))
        arrive(core[3:5])
        yield 2

    def relay_a(t):
        arrive(da[t])
        if t < 3:
            da.append(send_a(t + 1))
        for s in (t + 1, 7 - t) if t < 3 else (4,):
            dya[s] = send_dya(s)

    def relay_y(*slots):
        for s in slots:
            arrive(dya[s])
            dyb[s] = send_dyb(s)

    def relay_d(t, along=None):
        arrive(along if t == 0 else dz[t - 1])
        dz.append(send_d(t))

    qa = [
        go(remote(q_ref, qbuf.at[1], qs.at[0], qr.at[0], yr)),
        go(remote(q_ref, qbuf.at[3], qs.at[1], qr.at[1], yl)),
    ]
    kv = [send_kv(0)]
    g = [send_g(0)]
    hy = [
        go(remote(gug.at[sp, last], gug.at[sp, last], hs.at[i - 1], hr.at[i - 1], device(0, i)))
        for i in (1, 3, 2)
    ]
    ya = {0: send_ya(0)}
    yb = {}
    h = []

    top[...] = jnp.full(top.shape, -1e30, F32)
    total[...] = jnp.zeros(total.shape, F32)
    acc[...] = jnp.zeros(acc.shape, F32)
    row = lax.broadcasted_iota(jnp.int32, (2 * HD, 128), 0)

    def lay_queries(src, slot):
        for j in range(length // 128):
            turned = src[j * 128 : (j + 1) * 128, :].astype(F32).T * (LOG2E * HD**-0.5)
            for m in range(2):
                at = slot * cols + j * 256 + m * 128
                kept = jnp.where((row < HD) if m == 0 else (row >= HD), turned, 0.0)
                high = kept.astype(BF16)
                qbd[0:128, at : at + 128] = high
                qbd[128:256, at : at + 128] = (kept - high.astype(F32)).astype(BF16)

    def stage(slots):
        for n, s in enumerate(slots):
            kb = kslot(s)[...]
            kk[n * length : (n + 1) * length, 0:128] = kb
            kk[n * length : (n + 1) * length, 128:256] = kb
            vv[n * length : (n + 1) * length, :] = vslot(s)[...]

    def attend(count, begin, end):
        keys = count * length

        def tile(i, carry):
            halves = [pl.ds(pl.multiple_of(i * cols + n * length, length), length) for n in range(2)]
            scores = [jnp.dot(kk[0:keys, :], qbd[:, at], preferred_element_type=F32) for at in halves]
            for at, score in zip(halves, scores):
                before = top[0:1, at]
                now = jnp.maximum(before, jnp.max(score, axis=0, keepdims=True))
                shifted = jnp.exp2(score - now)
                factor = jnp.exp2(before - now)
                top[0:1, at] = now
                total[0:1, at] = total[0:1, at] * factor + jnp.sum(shifted, axis=0, keepdims=True)
                acc[:, at] = acc[:, at] * factor + lax.dot_general(
                    vv[0:keys, :],
                    shifted.astype(BF16),
                    (((0,), (0,)), ((), ())),
                    preferred_element_type=F32,
                )
            return carry

        lax.fori_loop(begin, end, tile, 0)

    lay_queries(q_ref, 0)
    stage([0])
    attend(1, 0, 1)
    arrive(qa)
    low, high_rows = pl.ds(0, half), pl.ds(half, half)
    qb = [
        go(remote(qbuf.at[1, low], qbuf.at[2, low], qs.at[2], qr.at[2], yr)),
        go(remote(qbuf.at[3, high_rows], qbuf.at[2, high_rows], qs.at[3], qr.at[3], yl)),
    ]
    lay_queries(qbuf.at[1], 1)
    lay_queries(qbuf.at[3], 3)
    attend(1, 1, 2)
    attend(1, 3, 4)
    arrive(qb)
    lay_queries(qbuf.at[2], 2)
    attend(1, 2, 3)

    for t in range(1, 5):
        arrive(kv[t - 1])
        if t < 4:
            kv.append(send_kv(t))
        slots = [t, 8 - t] if t < 4 else [4]
        stage(slots)
        attend(len(slots), 0, 2)
        arrive(g[t - 1])
        if t < 4:
            g.append(send_g(t))
            for s in slots:
                ya[s] = send_ya(s)
            for s in (0,) if t == 1 else (t - 1, 9 - t):
                arrive(ya[s])
                yb[s] = send_yb(s)
            if t == 3:
                arrive(hy)
                h.append(send_h(0))
        else:
            along = [
                go(remote(dall.at[sp, late], dall.at[sp, late], ys.at[i - 1], yrr.at[i - 1], device(0, i)))
                for i in (1, 3, 2)
            ]
        attend(len(slots), 2, 4)

    for slot in range(4):
        for n in range(2):
            at = slice(slot * cols + n * length, slot * cols + (n + 1) * length)
            lse[0, 2 * slot + n : 2 * slot + n + 1, :] = top[0:1, at] + jnp.log2(total[0:1, at])
    stats = [
        go(remote(lse.at[0], lse.at[4 - i], ls.at[i - 1], lr.at[3 - i], device(0, i))) for i in (2, 1, 3)
    ]
    arrive(h[0])
    h.append(send_h(1))
    da.append(send_a(0))
    arrive(stats)
    weights = {}
    for slot in range(4):
        for n in range(2):
            logs = []
            for e in range(4):
                r = 2 * ((slot + e) % 4) + n
                logs.append(lse[e, r : r + 1, :])
            highest = jnp.maximum(jnp.maximum(logs[0], logs[1]), jnp.maximum(logs[2], logs[3]))
            shares = [jnp.exp2(v - highest) for v in logs]
            at = slice(slot * cols + n * length, slot * cols + (n + 1) * length)
            weights[slot, n] = shares[0] / ((shares[0] + shares[1] + shares[2] + shares[3]) * total[0:1, at])

    def mixture(slot, rows):
        out = []
        for j in range(length // 128):
            maps = []
            for m in range(2):
                at = j * 256 + m * 128
                w = weights[slot, at // length][:, at % length : at % length + 128]
                maps.append(acc[rows, slot * cols + at : slot * cols + at + 128] * w)
            out.append(maps[0] - lam_ref[0] * maps[1])
        return jnp.concatenate(out, axis=1)

    up_rows, low_rows = slice(0, 64), slice(64, 128)
    at_up, at_low = pl.ds(0, 64), pl.ds(64, 64)
    part[2, up_rows, :] = mixture(2, up_rows).astype(BF16)
    part[2, low_rows, :] = mixture(2, low_rows).astype(BF16)
    over = [
        go(remote(part.at[2, at_up], relay.at[0], ms.at[0], mr.at[0], yr)),
        go(remote(part.at[2, at_low], relay.at[1], ms.at[1], mr.at[1], yl)),
    ]
    part[3, low_rows, :] = mixture(3, low_rows).astype(BF16)
    part[1, up_rows, :] = mixture(1, up_rows).astype(BF16)
    ends = [
        go(remote(part.at[3, at_low], landed.at[0, at_low], ms.at[2], mr.at[2], yr)),
        go(remote(part.at[1, at_up], landed.at[1, at_up], ms.at[3], mr.at[3], yl)),
    ]
    third, firsts = mixture(3, up_rows), mixture(1, low_rows)
    arrive(over)
    part[3, up_rows, :] = (third + relay[0].astype(F32)).astype(BF16)
    part[1, low_rows, :] = (firsts + relay[1].astype(F32)).astype(BF16)
    ends += [
        go(remote(part.at[3, at_up], landed.at[0, at_up], ms.at[4], mr.at[4], yr)),
        go(remote(part.at[1, at_low], landed.at[1, at_low], ms.at[5], mr.at[5], yl)),
    ]
    ya[4] = send_ya(4)
    for s in (3, 5):
        arrive(ya[s])
        yb[s] = send_yb(s)
    dya[0] = send_dya(0)
    arrive(h[1])
    h.append(send_h(2))
    relay_a(0)
    relay_d(0, along)
    mixed = mixture(0, slice(0, 128))
    arrive(ends)
    mixed = mixed + (landed[0].astype(F32) + landed[1].astype(F32))
    spread = jnp.mean(mixed * mixed, axis=0, keepdims=True)
    normed = mixed * lax.rsqrt(spread + 1e-06)
    gain = gain_ref[...][None, :] * 0.8
    parts_of = [slice(n * half, (n + 1) * half) for n in range(2)]
    heads, rows_in = [], []
    for j in range(length // 128):
        at = slice(j * 128, (j + 1) * 128)
        hall[tp, at, :] = (normed[:, at].T * gain).astype(BF16)
        if (j + 1) * 128 % half == 0:
            n = len(heads)
            heads.append(gather(hall, n, n * half))
            next(heads[n])

    def project(dx, n):
        chip = (x + dx) % 4
        for core in range(2):
            w = pl.ds(pl.multiple_of((chip * 2 + core) * VD, VD), VD)
            am[parts_of[n], :] += jnp.dot(
                hall[chip * 2 + core, parts_of[n], :], ow_ref[w, :], preferred_element_type=F32
            )

    for n in range(2):
        project(next(heads[n]), n)
    arrive(h[2])
    h.append(send_h(3))
    arrive(ya[4])
    yb[4] = send_yb(4)
    relay_y(0)
    for n in range(2):
        next(heads[n])
    for step in range(2):
        for n in range(2):
            project(next(heads[n]), n)
    relay_a(1)
    relay_y(1, 7)
    relay_d(1)
    for n in range(2):
        project(next(heads[n]), n)
        nall[tp, parts_of[n], :] = (am[parts_of[n], :] * ng_ref[...][None, :]).astype(BF16)
        rows_in.append(gather(nall, 2 + n, n * half))
        next(rows_in[n])
    value = am[...]
    square = value * value
    square = square[:, 0:128] + square[:, 128:256]
    for j in range(length // 128):
        ssq[tp, j : j + 1, :] = jnp.sum(square[j * 128 : (j + 1) * 128, :].T, axis=0, keepdims=True)
    ssq[tp, length // 128 :, :] = jnp.zeros((8 - length // 128, 128), F32)
    tiny = [
        go(remote(ssq.at[tp], ssq.at[tp], ts.at[i - 1], tr.at[i - 1], (sp, (tp + i) % 8)))
        for i in range(1, 8)
    ]
    for s in range(8):
        arrive(yb[s])
    arrive(h[3])

    per_chip = 2 * width // units_rows

    def product(dx, n):
        chip = (x + dx) % 4
        a = jnp.concatenate([nall[chip * 2, parts_of[n], :], nall[chip * 2 + 1, parts_of[n], :]], axis=1)
        w = gug[pl.ds(chip * per_chip, per_chip)].reshape(2 * width, 2 * units)
        return jnp.dot(a, w, preferred_element_type=F32)

    for n in range(2):
        big[parts_of[n], :] = product(next(rows_in[n]), n)
    for n in range(2):
        next(rows_in[n])
    relay_a(2)
    relay_d(2)
    relay_y(2, 6)
    for step in range(2):
        for n in range(2):
            big[parts_of[n], :] += product(next(rows_in[n]), n)
    for n in range(2):
        big[parts_of[n], :] += product(next(rows_in[n]), n)
    relay_a(3)
    relay_y(3, 5)
    relay_d(3)
    arrive(tiny)
    squares = ssq[0]
    for i in range(1, 8):
        squares = squares + ssq[i]
    factor = lax.rsqrt(squares * (1.0 / D) + 1e-06)
    for j in range(length // 128):
        rows = slice(j * 128, (j + 1) * 128)
        column = jnp.broadcast_to(factor[j : j + 1, :], (128, 128)).T[:, 0:1]
        scaled = big[rows, :] * column
        gate = jnp.concatenate([scaled[:, 0:whole], scaled[:, 2 * whole : 2 * whole + rest]], axis=1)
        gpad[8 + j * 128 : 8 + (j + 1) * 128, :] = gate.astype(BF16).astype(F32)
        big[rows, whole:] = scaled[:, whole:]
    gedge[0] = gpad[8:24, :].astype(BF16)
    gedge[1] = gpad[8 + length - 16 : 8 + length, :].astype(BF16)
    edge = [
        go(remote(gedge.at[1], halo.at[0], es.at[0], er.at[0], after)),
        go(remote(gedge.at[0], halo.at[1], es.at[1], er.at[1], before_)),
    ]

    def convolve(j):
        rows = slice(j * 128, (j + 1) * 128)
        at = 8 + j * 128
        conv = (
            gpad[at - 1 : at + 127, :] * cw_ref[0:1, :]
            + gpad[at : at + 128, :] * cw_ref[1:2, :]
            + gpad[at + 1 : at + 129, :] * cw_ref[2:3, :]
            + cb_ref[...][None, :]
        )
        up = jnp.concatenate([big[rows, whole : 2 * whole], big[rows, 2 * whole + rest :]], axis=1)
        hid[rows, :] = (conv / (1.0 + jnp.exp(-conv)) * up).astype(BF16)

    for j in range(1, length // 128 - 1):
        convolve(j)
    relay_y(4)
    arrive(edge)
    gpad[7:8, :] = jnp.where(sp == 0, 0.0, halo[0].astype(F32)[15:16, :])
    gpad[8 + length : 9 + length, :] = jnp.where(sp == NZ * NY - 1, 0.0, halo[1].astype(F32)[0:1, :])
    convolve(0)
    convolve(length // 128 - 1)

    for s in range(8):
        arrive(dyb[s])
    arrive(dz[3])
    per = width // units_rows

    def down(target):
        w = dall[pl.ds(target * per, per)].reshape(width, units)
        return lax.dot_general(
            hid[...], w, (((1,), (1,)), ((), ())), preferred_element_type=F32
        )

    order = (2, 1, 3, 0)
    crossing = {}
    for dx in order:
        psib[dx] = down(((x + dx) % 4) * 2 + (1 - c)).astype(BF16)
        crossing[dx] = go(remote(psib.at[dx], rsib.at[dx], bs.at[dx], br.at[dx], sib))
    upper, lower = slice(0, half), slice(half, length)
    at_upper, at_lower = pl.ds(0, half), pl.ds(half, half)
    ends = []
    for dx in order:
        piece = down(((x + dx) % 4) * 2 + c)
        arrive([crossing[dx]])
        piece = piece + rsib[dx].astype(F32)
        if dx == 2:
            pout[2] = piece.astype(BF16)
            over = [
                go(remote(pout.at[2, at_upper], relayed.at[0], ps.at[0], pr.at[0], xr_)),
                go(remote(pout.at[2, at_lower], relayed.at[1], ps.at[1], pr.at[1], xl_)),
            ]
        elif dx == 1:
            pout[1, lower, :] = piece[lower, :].astype(BF16)
            ends.append(go(remote(pout.at[1, at_lower], rout.at[0, at_lower], ps.at[2], pr.at[2], xr_)))
            keep[0] = piece[upper, :]
        elif dx == 3:
            pout[3, upper, :] = piece[upper, :].astype(BF16)
            ends.append(go(remote(pout.at[3, at_upper], rout.at[1, at_upper], ps.at[3], pr.at[3], xl_)))
            keep[1] = piece[lower, :]
            arrive(over)
            pout[1, upper, :] = (keep[0] + relayed[0].astype(F32)).astype(BF16)
            ends.append(go(remote(pout.at[1, at_upper], rout.at[0, at_upper], ps.at[4], pr.at[4], xr_)))
            pout[3, lower, :] = (keep[1] + relayed[1].astype(F32)).astype(BF16)
            ends.append(go(remote(pout.at[3, at_lower], rout.at[1, at_lower], ps.at[5], pr.at[5], xl_)))
        else:
            am[...] += piece
    arrive(ends)
    out_ref[...] = (am[...] + (rout[0].astype(F32) + rout[1].astype(F32))).astype(BF16)
    for copy in started:
        copy.wait_send()


def layer(q, k, v, gate, up, lam, gain, resid, ow, ng, cw, cb, dw):
    length, width = resid.shape
    cols = 2 * length
    rows, units = gate.shape
    half = length // 2
    dma, vmem = pltpu.SemaphoreType.DMA, pltpu.VMEM
    scratch = dict(
        gug=vmem((NZ * NY, rows, 2 * units), BF16),
        kbuf=vmem((8, length, 128), BF16),
        vbuf=vmem((8, length, 128), BF16),
        qbuf=vmem((4, length, 128), BF16),
        kk=vmem((2 * length, 256), BF16),
        vv=vmem((2 * length, 128), BF16),
        qbd=vmem((256, 4 * cols), BF16),
        top=vmem((8, 4 * cols), F32),
        total=vmem((8, 4 * cols), F32),
        acc=vmem((VD, 4 * cols), F32),
        lse=vmem((4, 8, length), F32),
        part=vmem((4, VD, length), BF16),
        relay=vmem((2, VD // 2, length), BF16),
        landed=vmem((2, VD, length), BF16),
        hall=vmem((8, length, VD), BF16),
        nall=vmem((8, length, width), BF16),
        am=vmem((length, width), F32),
        ssq=vmem((8, 8, 128), F32),
        big=vmem((length, 2 * units), F32),
        gpad=vmem((length + 16, units), F32),
        gedge=vmem((2, 16, units), BF16),
        halo=vmem((2, 16, units), BF16),
        hid=vmem((length, units), BF16),
        dall=vmem((NZ * NY, *dw.shape), BF16),
        psib=vmem((4, length, width), BF16),
        rsib=vmem((4, length, width), BF16),
        pout=vmem((4, length, width), BF16),
        relayed=vmem((2, half, width), BF16),
        rout=vmem((2, length, width), BF16),
        keep=vmem((2, half, width), F32),
    )
    semaphores = dict(
        ks=(2, 4), kr=(8,), vs=(2, 4), vr=(8,), qs=(4,), qr=(4,), gs=(2, 4), gr=(2, 4),
        ya_s=(2, 8), ya_r=(2, 8), yb_s=(2, 8), yb_r=(2, 8), hs=(3,), hr=(3,), hz_s=(2, 4), hz_r=(2, 4),
        ls=(3,), lr=(3,), ms=(6,), mr=(6,), xs=(4, 4), xr=(4, 4), cs=(4, 5), cr=(4, 5), ts=(7,), tr=(7,),
        es=(2,), er=(2,), ys=(3,), yrr=(3,), zs=(2, 4), zrr=(2, 4), as_=(2, 4), ar=(2, 4),
        dya_s=(2, 8), dya_r=(2, 8), dyb_s=(2, 8), dyb_r=(2, 8), bs=(4,), br=(4,), ps=(6,), pr=(6,),
    )
    return pl.pallas_call(
        layer_kernel,
        name="layer",
        out_shape=jax.ShapeDtypeStruct((length, width), BF16),
        in_specs=[VMEM] * 5 + [SMEM] + [VMEM] * 7,
        out_specs=VMEM,
        scratch_shapes=dict(scratch, **{n: dma(shape) for n, shape in semaphores.items()}),
        compiler_params=pltpu.CompilerParams(
            collective_id=0, has_side_effects=True, vmem_limit_bytes=63 * 2**20
        ),
    )(q, k, v, gate, up, lam, gain, resid, ow, ng, cw, cb, dw)


def on_device(
    resid,
    queries,
    keys,
    values,
    mix_lambda,
    head_gain,
    out_weight,
    norm_gain,
    gate_weight,
    up_weight,
    conv_weight,
    conv_bias,
    down_weight,
):
    return layer(
        queries,
        keys,
        values,
        gate_weight,
        up_weight,
        mix_lambda,
        head_gain,
        resid,
        out_weight,
        norm_gain,
        conv_weight,
        conv_bias,
        down_weight.T,
    )


def solution(mesh):
    return jax.shard_map(
        on_device,
        mesh=mesh,
        in_specs=(
            P("sp", "tp"),
            P("sp", "tp"),
            P("sp", "tp"),
            P("sp", "tp"),
            P("tp"),
            P(),
            P(None, "tp"),
            P("tp"),
            P("sp", "tp"),
            P("sp", "tp"),
            P(None, "tp"),
            P("tp"),
            P("tp", "sp"),
        ),
        out_specs=P("sp", "tp"),
        check_vma=False,
    )
```

```python
import jax
import jax.numpy as jnp
from jax import lax
from jax.experimental import pallas as pl
from jax.experimental.pallas import tpu as pltpu
from jax.sharding import PartitionSpec as P

D = 2048
HD = 64
VD = 128
LOG2E = 1.4426950408889634
NZ = 8
NY = 4
F32 = jnp.float32
BF16 = jnp.bfloat16
MESH = pl.DeviceIdType.MESH
VMEM = pl.BlockSpec(memory_space=pltpu.VMEM)
ANY = pl.BlockSpec(memory_space=pl.ANY)
SMEM = pl.BlockSpec(memory_space=pltpu.SMEM)


def remote(src, dst, send, recv, device):
    return pltpu.make_async_remote_copy(
        src_ref=src, dst_ref=dst, send_sem=send, recv_sem=recv, device_id=device, device_id_type=MESH
    )


def meet(peers):
    barrier = pltpu.get_barrier_semaphore()
    for peer in peers:
        pl.semaphore_signal(barrier, inc=1, device_id=peer, device_id_type=MESH)
    pl.semaphore_wait(barrier, len(peers))


def layer_kernel(
    q_ref,
    k_ref,
    v_ref,
    gate_ref,
    up_ref,
    lam_ref,
    gain_ref,
    resid_ref,
    ow_ref,
    ng_ref,
    cw_ref,
    cb_ref,
    dw_ref,
    out_ref,
    *,
    gug,
    kbuf,
    vbuf,
    qbuf,
    kk,
    vv,
    qbd,
    top,
    total,
    acc,
    lse,
    part,
    relay,
    landed,
    hall,
    nall,
    am,
    ssq,
    big,
    gpad,
    gedge,
    halo,
    hid,
    dall,
    psib,
    rsib,
    pout,
    relayed,
    rout,
    keep,
    ks,
    kr,
    vs,
    vr,
    qs,
    qr,
    gs,
    gr,
    ya_s,
    ya_r,
    yb_s,
    yb_r,
    hs,
    hr,
    hz_s,
    hz_r,
    ls,
    lr,
    ms,
    mr,
    xs,
    xr,
    cs,
    cr,
    ts,
    tr,
    es,
    er,
    ys,
    yrr,
    zs,
    zrr,
    as_,
    ar,
    dya_s,
    dya_r,
    dyb_s,
    dyb_r,
    bs,
    br,
    ps,
    pr,
):
    sp, tp = lax.axis_index("sp"), lax.axis_index("tp")
    z, y = sp // NY, sp % NY
    length = q_ref.shape[0]
    cols = 2 * length
    half = length // 2
    units = gate_ref.shape[1]
    whole = units // 128 * 128
    rest = units - whole
    first = pl.ds(0, 48)
    last = pl.ds(48, 16)

    def index(dz, dy):
        return ((z + dz) % NZ) * NY + (y + dy) % NY

    def device(dz, dy):
        return (index(dz, dy), tp)

    zr, zl = device(1, 0), device(7, 0)
    yr, yl = device(0, 1), device(0, 3)
    gug[sp, :, 0:whole] = gate_ref[:, 0:whole]
    gug[sp, :, whole : 2 * whole] = up_ref[:, 0:whole]
    gug[sp, :, 2 * whole :] = jnp.concatenate([gate_ref[:, whole:], up_ref[:, whole:]], axis=1)
    dall[sp] = dw_ref[...]
    am[...] = resid_ref[...].astype(F32)
    x, c = tp // 2, tp % 2
    width = resid_ref.shape[1]
    units_rows = dw_ref.shape[0]

    def xdev(dx, other=0):
        return (sp, ((x + dx) % 4) * 2 + (c + other) % 2)

    xr_, xl_, sib = xdev(1), xdev(3), xdev(0, 1)
    after, before_ = ((sp + 1) % (NZ * NY), tp), ((sp + NZ * NY - 1) % (NZ * NY), tp)
    tp_peers = [(sp, (tp + i) % 8) for i in range(1, 8)]
    meet([zr, zl, yr, yl, device(0, 2)] + tp_peers + [after, before_])
    started = []

    def go(copy):
        copy.start()
        started.append(copy)
        return copy

    def arrive(copies):
        for copy in copies:
            copy.wait_recv()

    def kslot(s):
        return k_ref if s == 0 else kbuf.at[s]

    def vslot(s):
        return v_ref if s == 0 else vbuf.at[s]

    def send_kv(t):
        right, left = t, (8 - t) % 8
        out = [go(remote(kslot(right), kbuf.at[t + 1], ks.at[0, t], kr.at[t + 1], zr))]
        if t < 3:
            out.append(go(remote(kslot(left), kbuf.at[7 - t], ks.at[1, t], kr.at[7 - t], zl)))
            out.append(go(remote(vslot(right), vbuf.at[t + 1], vs.at[0, t], vr.at[t + 1], zr)))
        out.append(go(remote(vslot(left), vbuf.at[7 - t], vs.at[1, t], vr.at[7 - t], zl)))
        return out

    def source(s, rows):
        return gug.at[index(8 - s, 0), rows]

    def parts(s):
        return (pl.ds(0, 16), pl.ds(16, 32)) if s % 2 == 0 else (pl.ds(0, 32), pl.ds(32, 16))

    def send_g(t):
        right, left = t, (8 - t) % 8
        rows_r, rows_l = parts(0) if t == 3 else (first, first)
        return [
            go(remote(source(right, rows_r), gug.at[index(8 - right, 0), rows_r], gs.at[0, t], gr.at[0, t], zr)),
            go(remote(source(left, rows_l), gug.at[index(8 - left, 0), rows_l], gs.at[1, t], gr.at[1, t], zl)),
        ]

    def send_ya(s):
        dst = gug.at[index(8 - s, 0), first]
        return [
            go(remote(source(s, first), dst, ya_s.at[0, s], ya_r.at[0, s], yr)),
            go(remote(source(s, first), dst, ya_s.at[1, s], ya_r.at[1, s], yl)),
        ]

    def send_yb(s):
        rows_r, rows_l = parts(s)
        a = gug.at[index(8 - s, 3), rows_r]
        b = gug.at[index(8 - s, 1), rows_l]
        return [
            go(remote(a, a, yb_s.at[0, s], yb_r.at[0, s], yr)),
            go(remote(b, b, yb_s.at[1, s], yb_r.at[1, s], yl)),
        ]

    def send_h(t):
        right, left = ((z + 8 - t) % NZ) * NY, ((z + t) % NZ) * NY
        if t < 3:
            a, b = gug.at[pl.ds(right, NY), last], gug.at[pl.ds(left, NY), last]
        else:
            a, b = gug.at[pl.ds(right, 2), last], gug.at[pl.ds(left + 2, 2), last]
        return [
            go(remote(a, a, hz_s.at[0, t], hz_r.at[0, t], zr)),
            go(remote(b, b, hz_s.at[1, t], hz_r.at[1, t], zl)),
        ]

    da, dya, dyb, dz = [], {}, {}, []
    turn = units_rows // 2
    early, late = pl.ds(0, turn), pl.ds(turn, turn)
    upper_q, lower_q = pl.ds(0, turn // 2), pl.ds(turn // 2, turn // 2)

    def dsource(s, rows):
        return dall.at[index(8 - s, 0), rows]

    def send_a(t):
        right, left = t, (8 - t) % 8
        rows_r, rows_l = (upper_q, lower_q) if t == 3 else (early, early)
        return [
            go(remote(dsource(right, rows_r), dall.at[index(8 - right, 0), rows_r], as_.at[0, t], ar.at[0, t], zr)),
            go(remote(dsource(left, rows_l), dall.at[index(8 - left, 0), rows_l], as_.at[1, t], ar.at[1, t], zl)),
        ]

    def send_dya(s):
        dst = dall.at[index(8 - s, 0), early]
        return [
            go(remote(dsource(s, early), dst, dya_s.at[0, s], dya_r.at[0, s], yr)),
            go(remote(dsource(s, early), dst, dya_s.at[1, s], dya_r.at[1, s], yl)),
        ]

    def send_dyb(s):
        a = dall.at[index(8 - s, 3), upper_q]
        b = dall.at[index(8 - s, 1), lower_q]
        return [
            go(remote(a, a, dyb_s.at[0, s], dyb_r.at[0, s], yr)),
            go(remote(b, b, dyb_s.at[1, s], dyb_r.at[1, s], yl)),
        ]

    def send_d(t):
        right, left = ((z + 8 - t) % NZ) * NY, ((z + t) % NZ) * NY
        if t < 3:
            a, b = dall.at[pl.ds(right, NY), late], dall.at[pl.ds(left, NY), late]
        else:
            a, b = dall.at[pl.ds(right, 2), late], dall.at[pl.ds(left + 2, 2), late]
        return [
            go(remote(a, a, zs.at[0, t], zrr.at[0, t], zr)),
            go(remote(b, b, zs.at[1, t], zrr.at[1, t], zl)),
        ]

    quarter = half // 2

    def gather(stack, k, begin):
        here = pl.ds(begin, half)
        upper, lower = pl.ds(begin, quarter), pl.ds(begin + quarter, quarter)
        mine = stack.at[tp, here]
        one = [
            go(remote(mine, mine, xs.at[k, 0], xr.at[k, 0], xr_)),
            go(remote(mine, mine, xs.at[k, 1], xr.at[k, 1], xl_)),
        ]
        core = [go(remote(mine, mine, cs.at[k, 0], cr.at[k, 0], sib))]
        yield None
        arrive(core)
        yield 0
        left, right = ((x + 3) % 4) * 2 + c, ((x + 1) % 4) * 2 + c
        arrive(one[:1])
        two = [go(remote(stack.at[left, upper], stack.at[left, upper], xs.at[k, 2], xr.at[k, 2], xr_))]
        core.append(go(remote(stack.at[left, here], stack.at[left, here], cs.at[k, 1], cr.at[k, 1], sib)))
        arrive(one[1:])
        two.append(go(remote(stack.at[right, lower], stack.at[right, lower], xs.at[k, 3], xr.at[k, 3], xl_)))
        core.append(go(remote(stack.at[right, here], stack.at[right, here], cs.at[k, 2], cr.at[k, 2], sib)))
        yield None
        arrive(core[1:2])
        yield 3
        arrive(core[2:3])
        yield 1
        far = ((x + 2) % 4) * 2 + c
        arrive(two[:1])
        core.append(go(remote(stack.at[far, upper], stack.at[far, upper], cs.at[k, 3], cr.at[k, 3], sib)))
        arrive(two[1:])
        core.append(go(remote(stack.at[far, lower], stack.at[far, lower], cs.at[k, 4], cr.at[k, 4], sib)))
        arrive(core[3:5])
        yield 2

    def relay_a(t):
        arrive(da[t])
        if t < 3:
            da.append(send_a(t + 1))
        for s in (t + 1, 7 - t) if t < 3 else (4,):
            dya[s] = send_dya(s)

    def relay_y(*slots):
        for s in slots:
            arrive(dya[s])
            dyb[s] = send_dyb(s)

    def relay_d(t, along=None):
        arrive(along if t == 0 else dz[t - 1])
        dz.append(send_d(t))

    qa = [
        go(remote(q_ref, qbuf.at[1], qs.at[0], qr.at[0], yr)),
        go(remote(q_ref, qbuf.at[3], qs.at[1], qr.at[1], yl)),
    ]
    kv = [send_kv(0)]
    g = [send_g(0)]
    hy = [
        go(remote(gug.at[sp, last], gug.at[sp, last], hs.at[i - 1], hr.at[i - 1], device(0, i)))
        for i in (1, 3, 2)
    ]
    ya = {0: send_ya(0)}
    yb = {}
    h = []

    top[...] = jnp.full(top.shape, -1e30, F32)
    total[...] = jnp.zeros(total.shape, F32)
    acc[...] = jnp.zeros(acc.shape, F32)
    row = lax.broadcasted_iota(jnp.int32, (2 * HD, 128), 0)

    def lay_queries(src, slot):
        for j in range(length // 128):
            turned = src[j * 128 : (j + 1) * 128, :].astype(F32).T * (LOG2E * HD**-0.5)
            for m in range(2):
                at = slot * cols + j * 256 + m * 128
                kept = jnp.where((row < HD) if m == 0 else (row >= HD), turned, 0.0)
                high = kept.astype(BF16)
                qbd[0:128, at : at + 128] = high
                qbd[128:256, at : at + 128] = (kept - high.astype(F32)).astype(BF16)

    def stage(slots):
        for n, s in enumerate(slots):
            kb = kslot(s)[...]
            kk[n * length : (n + 1) * length, 0:128] = kb
            kk[n * length : (n + 1) * length, 128:256] = kb
            vv[n * length : (n + 1) * length, :] = vslot(s)[...]

    def attend(count, begin, end):
        keys = count * length

        def tile(i, carry):
            halves = [pl.ds(pl.multiple_of(i * cols + n * length, length), length) for n in range(2)]
            scores = [jnp.dot(kk[0:keys, :], qbd[:, at], preferred_element_type=F32) for at in halves]
            for at, score in zip(halves, scores):
                before = top[0:1, at]
                now = jnp.maximum(before, jnp.max(score, axis=0, keepdims=True))
                shifted = jnp.exp2(score - now)
                factor = jnp.exp2(before - now)
                top[0:1, at] = now
                total[0:1, at] = total[0:1, at] * factor + jnp.sum(shifted, axis=0, keepdims=True)
                acc[:, at] = acc[:, at] * factor + lax.dot_general(
                    vv[0:keys, :],
                    shifted.astype(BF16),
                    (((0,), (0,)), ((), ())),
                    preferred_element_type=F32,
                )
            return carry

        lax.fori_loop(begin, end, tile, 0)

    lay_queries(q_ref, 0)
    stage([0])
    attend(1, 0, 1)
    arrive(qa)
    low, high_rows = pl.ds(0, half), pl.ds(half, half)
    qb = [
        go(remote(qbuf.at[1, low], qbuf.at[2, low], qs.at[2], qr.at[2], yr)),
        go(remote(qbuf.at[3, high_rows], qbuf.at[2, high_rows], qs.at[3], qr.at[3], yl)),
    ]
    lay_queries(qbuf.at[1], 1)
    lay_queries(qbuf.at[3], 3)
    attend(1, 1, 2)
    attend(1, 3, 4)
    arrive(qb)
    lay_queries(qbuf.at[2], 2)
    attend(1, 2, 3)

    for t in range(1, 5):
        arrive(kv[t - 1])
        if t < 4:
            kv.append(send_kv(t))
        slots = [t, 8 - t] if t < 4 else [4]
        stage(slots)
        attend(len(slots), 0, 2)
        arrive(g[t - 1])
        if t < 4:
            g.append(send_g(t))
            for s in slots:
                ya[s] = send_ya(s)
            for s in (0,) if t == 1 else (t - 1, 9 - t):
                arrive(ya[s])
                yb[s] = send_yb(s)
            if t == 3:
                arrive(hy)
                h.append(send_h(0))
        else:
            along = [
                go(remote(dall.at[sp, late], dall.at[sp, late], ys.at[i - 1], yrr.at[i - 1], device(0, i)))
                for i in (1, 3, 2)
            ]
        attend(len(slots), 2, 4)

    for slot in range(4):
        for n in range(2):
            at = slice(slot * cols + n * length, slot * cols + (n + 1) * length)
            lse[0, 2 * slot + n : 2 * slot + n + 1, :] = top[0:1, at] + jnp.log2(total[0:1, at])
    stats = [
        go(remote(lse.at[0], lse.at[4 - i], ls.at[i - 1], lr.at[3 - i], device(0, i))) for i in (2, 1, 3)
    ]
    arrive(h[0])
    h.append(send_h(1))
    da.append(send_a(0))
    arrive(stats)
    weights = {}
    for slot in range(4):
        for n in range(2):
            logs = []
            for e in range(4):
                r = 2 * ((slot + e) % 4) + n
                logs.append(lse[e, r : r + 1, :])
            highest = jnp.maximum(jnp.maximum(logs[0], logs[1]), jnp.maximum(logs[2], logs[3]))
            shares = [jnp.exp2(v - highest) for v in logs]
            at = slice(slot * cols + n * length, slot * cols + (n + 1) * length)
            weights[slot, n] = shares[0] / ((shares[0] + shares[1] + shares[2] + shares[3]) * total[0:1, at])

    def mixture(slot, rows):
        out = []
        for j in range(length // 128):
            maps = []
            for m in range(2):
                at = j * 256 + m * 128
                w = weights[slot, at // length][:, at % length : at % length + 128]
                maps.append(acc[rows, slot * cols + at : slot * cols + at + 128] * w)
            out.append(maps[0] - lam_ref[0] * maps[1])
        return jnp.concatenate(out, axis=1)

    up_rows, low_rows = slice(0, 64), slice(64, 128)
    at_up, at_low = pl.ds(0, 64), pl.ds(64, 64)
    part[2, up_rows, :] = mixture(2, up_rows).astype(BF16)
    part[2, low_rows, :] = mixture(2, low_rows).astype(BF16)
    over = [
        go(remote(part.at[2, at_up], relay.at[0], ms.at[0], mr.at[0], yr)),
        go(remote(part.at[2, at_low], relay.at[1], ms.at[1], mr.at[1], yl)),
    ]
    part[3, low_rows, :] = mixture(3, low_rows).astype(BF16)
    part[1, up_rows, :] = mixture(1, up_rows).astype(BF16)
    ends = [
        go(remote(part.at[3, at_low], landed.at[0, at_low], ms.at[2], mr.at[2], yr)),
        go(remote(part.at[1, at_up], landed.at[1, at_up], ms.at[3], mr.at[3], yl)),
    ]
    third, firsts = mixture(3, up_rows), mixture(1, low_rows)
    arrive(over)
    part[3, up_rows, :] = (third + relay[0].astype(F32)).astype(BF16)
    part[1, low_rows, :] = (firsts + relay[1].astype(F32)).astype(BF16)
    ends += [
        go(remote(part.at[3, at_up], landed.at[0, at_up], ms.at[4], mr.at[4], yr)),
        go(remote(part.at[1, at_low], landed.at[1, at_low], ms.at[5], mr.at[5], yl)),
    ]
    ya[4] = send_ya(4)
    for s in (3, 5):
        arrive(ya[s])
        yb[s] = send_yb(s)
    dya[0] = send_dya(0)
    arrive(h[1])
    h.append(send_h(2))
    relay_a(0)
    relay_d(0, along)
    mixed = mixture(0, slice(0, 128))
    arrive(ends)
    mixed = mixed + (landed[0].astype(F32) + landed[1].astype(F32))
    spread = jnp.mean(mixed * mixed, axis=0, keepdims=True)
    normed = mixed * lax.rsqrt(spread + 1e-06)
    gain = gain_ref[...][None, :] * 0.8
    parts_of = [slice(n * half, (n + 1) * half) for n in range(2)]
    heads, rows_in = [], []
    for j in range(length // 128):
        at = slice(j * 128, (j + 1) * 128)
        hall[tp, at, :] = (normed[:, at].T * gain).astype(BF16)
        if (j + 1) * 128 % half == 0:
            n = len(heads)
            heads.append(gather(hall, n, n * half))
            next(heads[n])

    def project(dx, n):
        chip = (x + dx) % 4
        for core in range(2):
            w = pl.ds(pl.multiple_of((chip * 2 + core) * VD, VD), VD)
            am[parts_of[n], :] += jnp.dot(
                hall[chip * 2 + core, parts_of[n], :], ow_ref[w, :], preferred_element_type=F32
            )

    for n in range(2):
        project(next(heads[n]), n)
    for n in range(2):
        next(heads[n])
    arrive(h[2])
    h.append(send_h(3))
    arrive(ya[4])
    yb[4] = send_yb(4)
    relay_y(0)
    for step in range(2):
        for n in range(2):
            project(next(heads[n]), n)
    relay_a(1)
    relay_y(1, 7)
    relay_d(1)
    for n in range(2):
        project(next(heads[n]), n)
        nall[tp, parts_of[n], :] = (am[parts_of[n], :] * ng_ref[...][None, :]).astype(BF16)
        rows_in.append(gather(nall, 2 + n, n * half))
        next(rows_in[n])
    value = am[...]
    square = value * value
    square = square[:, 0:128] + square[:, 128:256]
    for j in range(length // 128):
        ssq[tp, j : j + 1, :] = jnp.sum(square[j * 128 : (j + 1) * 128, :].T, axis=0, keepdims=True)
    ssq[tp, length // 128 :, :] = jnp.zeros((8 - length // 128, 128), F32)
    tiny = [
        go(remote(ssq.at[tp], ssq.at[tp], ts.at[i - 1], tr.at[i - 1], (sp, (tp + i) % 8)))
        for i in range(1, 8)
    ]

    per_chip = 2 * width // units_rows

    def product(dx, n):
        chip = (x + dx) % 4
        a = jnp.concatenate([nall[chip * 2, parts_of[n], :], nall[chip * 2 + 1, parts_of[n], :]], axis=1)
        w = gug[pl.ds(chip * per_chip, per_chip)].reshape(2 * width, 2 * units)
        return jnp.dot(a, w, preferred_element_type=F32)

    for n in range(2):
        next(rows_in[n])
    for n in range(2):
        next(rows_in[n])
    relay_a(2)
    relay_d(2)
    relay_y(2, 6)
    for s in range(8):
        arrive(yb[s])
    arrive(h[3])
    for n in range(2):
        big[parts_of[n], :] = product(0, n)
    for step in range(2):
        for n in range(2):
            big[parts_of[n], :] += product(next(rows_in[n]), n)
    for n in range(2):
        big[parts_of[n], :] += product(next(rows_in[n]), n)
    relay_a(3)
    relay_y(3, 5)
    relay_d(3)
    arrive(tiny)
    squares = ssq[0]
    for i in range(1, 8):
        squares = squares + ssq[i]
    factor = lax.rsqrt(squares * (1.0 / D) + 1e-06)
    for j in range(length // 128):
        rows = slice(j * 128, (j + 1) * 128)
        column = jnp.broadcast_to(factor[j : j + 1, :], (128, 128)).T[:, 0:1]
        scaled = big[rows, :] * column
        gate = jnp.concatenate([scaled[:, 0:whole], scaled[:, 2 * whole : 2 * whole + rest]], axis=1)
        gpad[8 + j * 128 : 8 + (j + 1) * 128, :] = gate.astype(BF16).astype(F32)
        big[rows, whole:] = scaled[:, whole:]
    gedge[0] = gpad[8:24, :].astype(BF16)
    gedge[1] = gpad[8 + length - 16 : 8 + length, :].astype(BF16)
    edge = [
        go(remote(gedge.at[1], halo.at[0], es.at[0], er.at[0], after)),
        go(remote(gedge.at[0], halo.at[1], es.at[1], er.at[1], before_)),
    ]

    def convolve(j):
        rows = slice(j * 128, (j + 1) * 128)
        at = 8 + j * 128
        conv = (
            gpad[at - 1 : at + 127, :] * cw_ref[0:1, :]
            + gpad[at : at + 128, :] * cw_ref[1:2, :]
            + gpad[at + 1 : at + 129, :] * cw_ref[2:3, :]
            + cb_ref[...][None, :]
        )
        up = jnp.concatenate([big[rows, whole : 2 * whole], big[rows, 2 * whole + rest :]], axis=1)
        hid[rows, :] = (conv / (1.0 + jnp.exp(-conv)) * up).astype(BF16)

    for j in range(1, length // 128 - 1):
        convolve(j)
    relay_y(4)
    arrive(edge)
    gpad[7:8, :] = jnp.where(sp == 0, 0.0, halo[0].astype(F32)[15:16, :])
    gpad[8 + length : 9 + length, :] = jnp.where(sp == NZ * NY - 1, 0.0, halo[1].astype(F32)[0:1, :])
    convolve(0)
    convolve(length // 128 - 1)

    for s in range(8):
        arrive(dyb[s])
    arrive(dz[3])
    per = width // units_rows

    def down(target):
        w = dall[pl.ds(target * per, per)].reshape(width, units)
        return lax.dot_general(
            hid[...], w, (((1,), (1,)), ((), ())), preferred_element_type=F32
        )

    order = (2, 1, 3, 0)
    crossing = {}
    for dx in order:
        psib[dx] = down(((x + dx) % 4) * 2 + (1 - c)).astype(BF16)
        crossing[dx] = go(remote(psib.at[dx], rsib.at[dx], bs.at[dx], br.at[dx], sib))
    upper, lower = slice(0, half), slice(half, length)
    at_upper, at_lower = pl.ds(0, half), pl.ds(half, half)
    ends = []
    for dx in order:
        piece = down(((x + dx) % 4) * 2 + c)
        arrive([crossing[dx]])
        piece = piece + rsib[dx].astype(F32)
        if dx == 2:
            pout[2] = piece.astype(BF16)
            over = [
                go(remote(pout.at[2, at_upper], relayed.at[0], ps.at[0], pr.at[0], xr_)),
                go(remote(pout.at[2, at_lower], relayed.at[1], ps.at[1], pr.at[1], xl_)),
            ]
        elif dx == 1:
            pout[1, lower, :] = piece[lower, :].astype(BF16)
            ends.append(go(remote(pout.at[1, at_lower], rout.at[0, at_lower], ps.at[2], pr.at[2], xr_)))
            keep[0] = piece[upper, :]
        elif dx == 3:
            pout[3, upper, :] = piece[upper, :].astype(BF16)
            ends.append(go(remote(pout.at[3, at_upper], rout.at[1, at_upper], ps.at[3], pr.at[3], xl_)))
            keep[1] = piece[lower, :]
            arrive(over)
            pout[1, upper, :] = (keep[0] + relayed[0].astype(F32)).astype(BF16)
            ends.append(go(remote(pout.at[1, at_upper], rout.at[0, at_upper], ps.at[4], pr.at[4], xr_)))
            pout[3, lower, :] = (keep[1] + relayed[1].astype(F32)).astype(BF16)
            ends.append(go(remote(pout.at[3, at_lower], rout.at[1, at_lower], ps.at[5], pr.at[5], xl_)))
        else:
            am[...] += piece
    arrive(ends)
    out_ref[...] = (am[...] + (rout[0].astype(F32) + rout[1].astype(F32))).astype(BF16)
    for copy in started:
        copy.wait_send()


def layer(q, k, v, gate, up, lam, gain, resid, ow, ng, cw, cb, dw):
    length, width = resid.shape
    cols = 2 * length
    rows, units = gate.shape
    half = length // 2
    dma, vmem = pltpu.SemaphoreType.DMA, pltpu.VMEM
    scratch = dict(
        gug=vmem((NZ * NY, rows, 2 * units), BF16),
        kbuf=vmem((8, length, 128), BF16),
        vbuf=vmem((8, length, 128), BF16),
        qbuf=vmem((4, length, 128), BF16),
        kk=vmem((2 * length, 256), BF16),
        vv=vmem((2 * length, 128), BF16),
        qbd=vmem((256, 4 * cols), BF16),
        top=vmem((8, 4 * cols), F32),
        total=vmem((8, 4 * cols), F32),
        acc=vmem((VD, 4 * cols), F32),
        lse=vmem((4, 8, length), F32),
        part=vmem((4, VD, length), BF16),
        relay=vmem((2, VD // 2, length), BF16),
        landed=vmem((2, VD, length), BF16),
        hall=vmem((8, length, VD), BF16),
        nall=vmem((8, length, width), BF16),
        am=vmem((length, width), F32),
        ssq=vmem((8, 8, 128), F32),
        big=vmem((length, 2 * units), F32),
        gpad=vmem((length + 16, units), F32),
        gedge=vmem((2, 16, units), BF16),
        halo=vmem((2, 16, units), BF16),
        hid=vmem((length, units), BF16),
        dall=vmem((NZ * NY, *dw.shape), BF16),
        psib=vmem((4, length, width), BF16),
        rsib=vmem((4, length, width), BF16),
        pout=vmem((4, length, width), BF16),
        relayed=vmem((2, half, width), BF16),
        rout=vmem((2, length, width), BF16),
        keep=vmem((2, half, width), F32),
    )
    semaphores = dict(
        ks=(2, 4), kr=(8,), vs=(2, 4), vr=(8,), qs=(4,), qr=(4,), gs=(2, 4), gr=(2, 4),
        ya_s=(2, 8), ya_r=(2, 8), yb_s=(2, 8), yb_r=(2, 8), hs=(3,), hr=(3,), hz_s=(2, 4), hz_r=(2, 4),
        ls=(3,), lr=(3,), ms=(6,), mr=(6,), xs=(4, 4), xr=(4, 4), cs=(4, 5), cr=(4, 5), ts=(7,), tr=(7,),
        es=(2,), er=(2,), ys=(3,), yrr=(3,), zs=(2, 4), zrr=(2, 4), as_=(2, 4), ar=(2, 4),
        dya_s=(2, 8), dya_r=(2, 8), dyb_s=(2, 8), dyb_r=(2, 8), bs=(4,), br=(4,), ps=(6,), pr=(6,),
    )
    return pl.pallas_call(
        layer_kernel,
        name="layer",
        out_shape=jax.ShapeDtypeStruct((length, width), BF16),
        in_specs=[VMEM] * 5 + [SMEM] + [VMEM] * 7,
        out_specs=VMEM,
        scratch_shapes=dict(scratch, **{n: dma(shape) for n, shape in semaphores.items()}),
        compiler_params=pltpu.CompilerParams(
            collective_id=0, has_side_effects=True, vmem_limit_bytes=63 * 2**20
        ),
    )(q, k, v, gate, up, lam, gain, resid, ow, ng, cw, cb, dw)


def on_device(
    resid,
    queries,
    keys,
    values,
    mix_lambda,
    head_gain,
    out_weight,
    norm_gain,
    gate_weight,
    up_weight,
    conv_weight,
    conv_bias,
    down_weight,
):
    return layer(
        queries,
        keys,
        values,
        gate_weight,
        up_weight,
        mix_lambda,
        head_gain,
        resid,
        out_weight,
        norm_gain,
        conv_weight,
        conv_bias,
        down_weight.T,
    )


def solution(mesh):
    return jax.shard_map(
        on_device,
        mesh=mesh,
        in_specs=(
            P("sp", "tp"),
            P("sp", "tp"),
            P("sp", "tp"),
            P("sp", "tp"),
            P("tp"),
            P(),
            P(None, "tp"),
            P("tp"),
            P("sp", "tp"),
            P("sp", "tp"),
            P(None, "tp"),
            P("tp"),
            P("tp", "sp"),
        ),
        out_specs=P("sp", "tp"),
        check_vma=False,
    )
```
